32 devices in a mesh: rep: 2 (over x), fs: 8 (over z, y), tp: 2 (over core).
Axes of the slice: x: 2, y: 2, z: 4, core: 2. Of those that a mesh axis runs over, the one named last changes fastest.
Arguments:
- inputs: bfloat16 [2048, 2048], P(('rep', 'fs'), 'tp'), may hold values from -6 to 6
- cotangent: bfloat16 [2048, 2048], P(('rep', 'fs'), 'tp'), may hold values from -8 to 8
- gate_weight: bfloat16 [2048, 2816], P('fs', 'tp'), may hold values from -0.125 to 0.125
- up_weight: bfloat16 [2048, 2816], P('fs', 'tp'), may hold values from -0.125 to 0.125
- down_weight: bfloat16 [2816, 2048], P('tp', 'fs'), may hold values from -0.109375 to 0.109375
Outputs:
- grad_inputs: bfloat16 [2048, 2048], P(('rep', 'fs'), 'tp')
- grad_gate_weight: float32 [2048, 2816], P('fs', 'tp')
- grad_up_weight: float32 [2048, 2816], P('fs', 'tp')
- grad_down_weight: float32 [2816, 2048], P('tp', 'fs')
The draws below stay inside these ranges and needn't reach their ends.
All inputs are finite; a program needn't handle non-finite values.
Results may differ from the reference program's by a relative error of at most 0.014.
Values may be sent and summed in bfloat16 or wider, within the bound.
A program may use at most 64 MiB of HBM per device.

```python
import jax
import jax.numpy as jnp
from jax import lax

D = 2048
FF = 2816
TOKENS = 2048
N_TP = 2


def strengthened(result, rng, source, target, blocks, factor):
    def block_of(position):
        return (jnp.arange(result.shape[position]) // (result.shape[position] // blocks)).reshape((-1,) + (1,) * (result.ndim - 1 - position))

    one_side = jax.random.permutation(rng, blocks)[block_of(target)]
    other_side = (block_of(target) + blocks // 2) % blocks
    return jnp.where((block_of(source) == one_side) | (block_of(source) == other_side), factor * result, result)


def block_scale(rng, shape, split, least, top_value):
    def one(axis_at, shards_of):
        steps = jax.random.uniform(jax.random.fold_in(jax.random.fold_in(rng, 6), axis_at), (shards_of,), jnp.float32, least / len(split), top_value / len(split))
        return jnp.repeat(jnp.exp(steps), shape[axis_at] // shards_of).reshape((-1,) + (1,) * (len(shape) - axis_at - 1))

    loudness = one(*split[0])
    for cut in split[1:]:
        loudness = loudness * one(*cut)
    return loudness


def noise(stream_key, extent, deviation, reach, shards=(), kind=jnp.bfloat16):
    drawn = deviation * jax.random.normal(stream_key, extent, jnp.float32)
    if shards:
        drawn = drawn * block_scale(stream_key, extent, shards, -0.22, 0.18)
    return jnp.clip(drawn, -reach, reach).astype(kind)


def gaussian_with(own_key, extent, spread, bound, shards, heavy, held_as=jnp.bfloat16):
    drawn = spread * jax.random.normal(own_key, extent, jnp.float32)
    if shards:
        drawn = drawn * block_scale(own_key, extent, shards, -0.22, 0.18)
    return jnp.clip(strengthened(drawn, jax.random.fold_in(own_key, 3), *heavy), -bound, bound).astype(held_as)


def setup_inputs(seed: int = 0) -> dict:
    streams_of = jax.random.split(jax.random.key(seed), 6)
    return {
        "inputs": noise(streams_of[0], (TOKENS, D), 1.0, 6.0, ((0, 16), (1, 2))),
        "cotangent": gaussian_with(streams_of[1], (TOKENS, D), 1.0, 8.0, ((0, 16), (1, 2)), (0, 1, 16, 2.0)),
        "gate_weight": noise(streams_of[2], (D, FF), D ** -0.5, 0.125, ((0, 8), (1, 2))),
        "up_weight": noise(streams_of[3], (D, FF), D ** -0.5, 0.125, ((0, 8), (1, 2))),
        "down_weight": noise(streams_of[4], (FF, D), FF ** -0.5, 0.109375, ((0, 2), (1, 8))),
    }


def reference(inputs, cotangent, gate_weight, up_weight, down_weight):
    gate_pre = jnp.dot(inputs, gate_weight, preferred_element_type=jnp.float32)
    up_pre = jnp.dot(inputs, up_weight, preferred_element_type=jnp.float32)
    sigmoid_gate = jax.nn.sigmoid(gate_pre)
    activated = gate_pre * sigmoid_gate
    hidden = (activated * up_pre).astype(jnp.bfloat16)
    grad_hidden = jnp.dot(cotangent, down_weight.T, preferred_element_type=jnp.float32)
    grad_gate = (grad_hidden * up_pre * sigmoid_gate * (1.0 + gate_pre * (1.0 - sigmoid_gate))).astype(jnp.bfloat16)
    grad_up = (grad_hidden * activated).astype(jnp.bfloat16)
    grad_down_weight = jnp.dot(hidden.T, cotangent, preferred_element_type=jnp.float32)
    grad_gate_weight = jnp.dot(inputs.T, grad_gate, preferred_element_type=jnp.float32)
    grad_up_weight = jnp.dot(inputs.T, grad_up, preferred_element_type=jnp.float32)
    block_units = FF // N_TP
    running = jnp.zeros(inputs.shape, jnp.float32)
    for index in range(N_TP):
        lower = index * block_units
        upper = lower + block_units
        partial_sum = jnp.dot(grad_gate[:, lower:upper], gate_weight[:, lower:upper].T, preferred_element_type=jnp.float32)
        partial_sum = partial_sum + jnp.dot(grad_up[:, lower:upper], up_weight[:, lower:upper].T, preferred_element_type=jnp.float32)
        rounded = lax.optimization_barrier(partial_sum.astype(jnp.bfloat16))
        running = running + rounded.astype(jnp.float32)
    grad_inputs = running.astype(jnp.bfloat16)
    return (grad_inputs, grad_gate_weight, grad_up_weight, grad_down_weight)
```

```python
import functools

import jax
import jax.numpy as jnp
from jax import lax
from jax.experimental import pallas as pl
from jax.experimental.pallas import tpu as pltpu
from jax.sharding import PartitionSpec as P

MESH = pl.DeviceIdType.MESH


def enter(n_rep, n_fs, n_tp):
    barrier = pltpu.get_barrier_semaphore()
    for axis, n in (("rep", n_rep), ("fs", n_fs), ("tp", n_tp)):
        me = lax.axis_index(axis)
        for k in range(1, n):
            pl.semaphore_signal(
                barrier, inc=1, device_id={axis: lax.rem(me + k, n)}, device_id_type=MESH
            )
    pl.semaphore_wait(barrier, n_rep + n_fs + n_tp - 3)


class Sender:
    def __init__(self, sems):
        self.sems, self.used, self.pending = sems, 0, []

    def run(self, build, when):
        if when is None:
            build().start()
        else:
            pl.when(when)(lambda: build().start())

    def send(self, src, dst, recv_sem, axis, peer, when=None):
        def build(at=self.used):
            return pltpu.make_async_remote_copy(
                src_ref=src,
                dst_ref=dst,
                send_sem=self.sems.at[at],
                recv_sem=recv_sem,
                device_id={axis: peer},
                device_id_type=MESH,
            )

        self.used += 1
        self.run(build, when)
        self.pending.append((lambda: build().wait_send(), when))

    def local(self, src, dst):
        def build(at=self.used):
            return pltpu.make_async_copy(src, dst, self.sems.at[at])

        self.used += 1
        self.run(build, None)
        self.pending.append((lambda: build().wait(), None))

    def finish(self):
        for wait, when in self.pending:
            if when is None:
                wait()
            else:
                pl.when(when)(wait)


def arrived(slot, recv_sem, when=None):
    def wait():
        pltpu.make_async_copy(slot, slot, recv_sem).wait()

    if when is None:
        wait()
    else:
        pl.when(when)(wait)


def near_first(n):
    return sorted(range(1, n), key=lambda k: min(k, n - k))


def layer_kernel(
    sizes, x_ref, c_ref, gate_ref, up_ref, down_ref, dx_ref, dw_ref,
    xa, ca, wt, wa, pre, gt, ht, p, p_in, q, x_in, r, z_in, gp, go, g_in, gs,
    sends, act_recv, w_recv, p_recv, x_recv, z_recv, g_recv, d_recv,
):
    n_rep, n_fs, n_tp, n_y = sizes
    n_z = n_fs // n_y
    f32, bf16 = jnp.float32, jnp.bfloat16
    rep, fs, tp = (lax.axis_index(axis) for axis in ("rep", "fs", "tp"))
    z, y = fs // n_y, lax.rem(fs, n_y)
    tokens, width = x_ref.shape
    units, depth = wa.shape[1], down_ref.shape[1]
    group = n_z * tokens
    near = near_first(n_z)
    out = Sender(sends)
    enter(n_rep, n_fs, n_tp)

    def span(at, size):
        return pl.ds(pl.multiple_of(at * size, size), size)

    def peers(me, n):
        return [lax.rem(me + k, n) for k in range(1, n)]

    def at_z(other, row=y):
        return other * n_y + row

    own_acts, acts = (x_ref, c_ref), (xa, ca)

    def act_slot(a, shard, part):
        return acts[a].at[span(shard, tokens), span(part, width)]

    def act_send(a, shard, src, axis, peer, when=None):
        out.send(src, act_slot(a, shard, tp), act_recv.at[a, shard, tp], axis, peer, when)

    def to_rep(a, shard, src, when=None):
        for peer in peers(rep, n_rep):
            act_send(a, shard, src, "rep", peer, when)

    def to_tp(a, shard, src, when=None):
        for peer in peers(tp, n_tp):
            act_send(a, shard, src, "tp", peer, when)

    def from_rep(other):
        for peer in peers(rep, n_rep):
            for a in range(2):
                shard = peer * n_z + other
                slot = act_slot(a, shard, tp)
                arrived(slot, act_recv.at[a, shard, tp])
                to_tp(a, shard, slot)

    mine = rep * n_z + z
    for a in range(2):
        act_send(a, mine, own_acts[a], "fs", fs + n_y, z + 1 < n_z)
        act_send(a, mine, own_acts[a], "fs", fs - n_y, z >= 1)
        to_rep(a, mine, own_acts[a])
    for a in range(2):
        to_tp(a, mine, own_acts[a])

    wt[0] = gate_ref[...].T
    wt[1] = up_ref[...].T

    def w_part(i, owner):
        rows = span(owner, units)
        return down_ref.at[rows] if i == 2 else wt.at[i, rows]

    def w_slot(i, block):
        return wa.at[i, :, span(block, depth)]

    def w_send(i, block, src, peer):
        out.send(src, w_slot(i, block), w_recv.at[i, block], "fs", peer)

    for i in range(3):
        for row in peers(y, n_y):
            w_send(i, fs, w_part(i, mine), at_z(z, row))
    for i in range(3):
        wa[i, :, span(fs, depth)] = w_part(i, mine)[...]
    for a in range(2):
        acts[a][span(mine, tokens), span(tp, width)] = own_acts[a][...]

    def send_weights():
        for k in reversed(near):
            other = lax.rem(z + k, n_z)
            for i in range(3):
                w_send(i, fs, w_part(i, rep * n_z + other), at_z(other))

    for k in range(1, n_z):
        for a in range(2):
            for here, onward, step in ((z >= k, z + 1 < n_z, -1), (z + k < n_z, z >= 1, 1)):
                shard = mine + step * k
                slot = act_slot(a, shard, tp)
                arrived(slot, act_recv.at[a, shard, tp], here)
                if k < n_z - 1:
                    act_send(a, shard, slot, "fs", fs - step * n_y, jnp.logical_and(here, onward))
                to_rep(a, shard, slot, here)
                to_tp(a, shard, slot, here)
        if k == max(1, n_z - 2):
            send_weights()
        if k == 1:
            from_rep(z)
    if n_z == 1:
        from_rep(z)
    for k in near:
        other = lax.rem(z + n_z - k, n_z)
        for i in range(3):
            slot = w_slot(i, at_z(other))
            arrived(slot, w_recv.at[i, at_z(other)])
            for row in peers(y, n_y):
                w_send(i, at_z(other), slot, at_z(z, row))
        from_rep(other)
    for k in range(n_z):
        other = lax.rem(z + k, n_z)
        for i in range(3):
            for row in peers(y, n_y):
                arrived(w_slot(i, at_z(other, row)), w_recv.at[i, at_z(other, row)])
    for part in peers(tp, n_tp):
        for shard in range(n_rep * n_z):
            for a in range(2):
                arrived(act_slot(a, shard, part), act_recv.at[a, shard, part])

    last = (((1,), (1,)), ((), ()))
    first = (((0,), (0,)), ((), ()))

    def forward(side):
        cols = span(side, group)
        for i in range(3):
            pre[i] = lax.dot_general(
                wa[i], acts[i // 2][cols], last, preferred_element_type=f32
            )

        @pl.loop(0, units // 16)
        def _(step):
            rows, more = span(step, 16), pl.ds(pl.multiple_of(units + step * 16, 16), 16)
            gate_pre, up_pre, grad_hidden = pre[0, rows], pre[1, rows], pre[2, rows]
            sigmoid_gate = jax.nn.sigmoid(gate_pre)
            activated = gate_pre * sigmoid_gate
            ht[rows, cols] = (activated * up_pre).astype(bf16)
            gt[rows, cols] = (
                grad_hidden * up_pre * sigmoid_gate * (1.0 + gate_pre * (1.0 - sigmoid_gate))
            ).astype(bf16)
            gt[more, cols] = (grad_hidden * activated).astype(bf16)

    def partial_inputs(side):
        rows = span(side, group)
        w_in = wa[0:2].reshape(2 * units, wa.shape[2])
        p[rows] = lax.dot_general(gt[:, rows], w_in, first, preferred_element_type=f32).astype(bf16)
        for k in range(n_z):
            shard = side * n_z + lax.rem(z + k, n_z)
            for j in range(1, n_tp):
                peer = lax.rem(tp + j, n_tp)
                out.send(
                    p.at[span(shard, tokens), span(peer, width)],
                    p_in.at[j - 1, shard],
                    p_recv.at[j - 1, shard],
                    "tp",
                    peer,
                )

    def pair_sum(shard):
        total = p[span(shard, tokens), span(tp, width)].astype(f32)
        for j in range(n_tp - 1):
            arrived(p_in.at[j, shard], p_recv.at[j, shard])
            total = total + p_in[j, shard].astype(f32)
        return total

    def weight_block(block, dst):
        cols = span(block, depth)
        dst[0:2] = jnp.dot(gt[...], xa[:, cols], preferred_element_type=f32).astype(
            dst.dtype
        ).reshape(2, units, depth)
        dst[2] = jnp.dot(ht[...], ca[:, cols], preferred_element_type=f32).astype(dst.dtype)

    order = near + [0]
    for j in range(1, n_rep):
        side = lax.rem(rep + j, n_rep)
        forward(side)
        partial_inputs(side)
    forward(rep)
    for k in order:
        other = lax.rem(z + k, n_z)
        for j in range(1, n_rep):
            side = lax.rem(rep + j, n_rep)
            q[j - 1, other] = pair_sum(side * n_z + other).astype(bf16)
            out.send(
                q.at[j - 1, other], x_in.at[j - 1, other], x_recv.at[j - 1, other], "rep", side
            )
    for k in order:
        other = lax.rem(z + k, n_z)
        for j in range(1, n_y):
            row = lax.rem(y + j, n_y)
            weight_block(at_z(other, row), gp.at[j - 1, other])
            out.send(
                gp.at[j - 1, other], g_in.at[j - 1, other], g_recv.at[j - 1, other],
                "fs", at_z(z, row),
            )
    partial_inputs(rep)
    for k in order:
        other = lax.rem(z + k, n_z)
        weight_block(at_z(other), go.at[other])

    def dw_slot(side, other):
        return dw_ref.at[:, span(side * n_z + other, units)]

    def dw_send(other, src):
        for peer in peers(rep, n_rep):
            out.send(src, dw_slot(rep, other), d_recv.at[rep, other], "rep", peer)

    def x_step(k):
        other = lax.rem(z + k, n_z)
        total = pair_sum(mine - z + other)
        for j in range(n_rep - 1):
            arrived(x_in.at[j, other], x_recv.at[j, other])
            total = total + x_in[j, other].astype(f32)
        if k:
            r[other] = total.astype(bf16)
            out.send(r.at[other], z_in.at[z], z_recv.at[z], "fs", at_z(other))
        else:
            z_in[z] = total.astype(bf16)

    def g_step(k):
        other = lax.rem(z + k, n_z)
        total = go[other]
        for j in range(n_y - 1):
            arrived(g_in.at[j, other], g_recv.at[j, other])
            total = total + g_in[j, other].astype(f32)
        gs[other] = total.astype(bf16)
        if k:
            out.send(gs.at[other], dw_slot(rep, z), d_recv.at[rep, z], "fs", at_z(other))
        else:
            dw_send(z, gs.at[z])
            dw_ref[:, span(mine, units)] = gs[z]

    def g_forward(k):
        other = lax.rem(z + n_z - k, n_z)
        arrived(dw_slot(rep, other), d_recv.at[rep, other])
        dw_send(other, dw_slot(rep, other))

    for k in order:
        x_step(k)
        g_step(k)
    for k in near:
        g_forward(k)
    total = z_in[z].astype(f32)
    for k in near:
        other = lax.rem(z + n_z - k, n_z)
        arrived(z_in.at[other], z_recv.at[other])
        total = total + z_in[other].astype(f32)
    dx_ref[...] = total.astype(bf16)
    for side in peers(rep, n_rep):
        for k in range(n_z):
            other = lax.rem(z + n_z - k, n_z)
            arrived(dw_slot(side, other), d_recv.at[side, other])
    out.finish()


VMEM = pl.BlockSpec(memory_space=pltpu.VMEM)
DMA = pltpu.SemaphoreType.DMA


def fused(sizes, x, c, gate_weight, up_weight, down_weight):
    bf16, f32 = jnp.bfloat16, jnp.float32
    n_rep, n_fs, n_tp, n_y = sizes
    n_z = n_fs // n_y
    tokens, width = x.shape
    depth, hidden_tp = gate_weight.shape
    model, units = width * n_tp, hidden_tp // (n_rep * n_z)
    shards = n_rep * n_z
    group = shards * tokens
    grad_inputs, dw = pl.pallas_call(
        functools.partial(layer_kernel, sizes),
        out_shape=(
            jax.ShapeDtypeStruct((tokens, width), bf16),
            jax.ShapeDtypeStruct((3, hidden_tp, depth), bf16),
        ),
        in_specs=[VMEM] * 5,
        out_specs=(VMEM, VMEM),
        scratch_shapes=[
            pltpu.VMEM((group, model), bf16),
            pltpu.VMEM((group, model), bf16),
            pltpu.VMEM((2, hidden_tp, depth), bf16),
            pltpu.VMEM((3, units, model), bf16),
            pltpu.VMEM((3, units, n_z * tokens), f32),
            pltpu.VMEM((2 * units, group), bf16),
            pltpu.VMEM((units, group), bf16),
            pltpu.VMEM((group, model), bf16),
            pltpu.VMEM((n_tp - 1, shards, tokens, width), bf16),
            pltpu.VMEM((n_rep - 1, n_z, tokens, width), bf16),
            pltpu.VMEM((n_rep - 1, n_z, tokens, width), bf16),
            pltpu.VMEM((n_z, tokens, width), bf16),
            pltpu.VMEM((n_z, tokens, width), bf16),
            pltpu.VMEM((n_y - 1, n_z, 3, units, depth), bf16),
            pltpu.VMEM((n_z, 3, units, depth), f32),
            pltpu.VMEM((n_y - 1, n_z, 3, units, depth), bf16),
            pltpu.VMEM((n_z, 3, units, depth), bf16),
            DMA((256,)),
            DMA((2, shards, n_tp)),
            DMA((3, n_fs)),
            DMA((n_tp - 1, shards)),
            DMA((n_rep - 1, n_z)),
            DMA((n_z,)),
            DMA((n_y - 1, n_z)),
            DMA((n_rep, n_z)),
        ],
        compiler_params=pltpu.CompilerParams(
            collective_id=0, has_side_effects=True, vmem_limit_bytes=60 * 2**20
        ),
    )(x, c, gate_weight, up_weight, down_weight)
    return grad_inputs, dw[0].T.astype(f32), dw[1].T.astype(f32), dw[2].astype(f32)


def gathered(x, c, gate_weight, up_weight, down_weight):
    bf16, f32 = jnp.bfloat16, jnp.float32
    last = (((1,), (1,)), ((), ()))
    first = (((0,), (0,)), ((), ()))
    x, c = (lax.all_gather(v, "tp", axis=1, tiled=True) for v in (x, c))
    gate, up = (lax.all_gather(v, "fs", axis=0, tiled=True) for v in (gate_weight, up_weight))
    down = lax.all_gather(down_weight, "fs", axis=1, tiled=True)
    gate_pre = jnp.dot(x, gate, preferred_element_type=f32)
    up_pre = jnp.dot(x, up, preferred_element_type=f32)
    grad_hidden = lax.dot_general(c, down, last, preferred_element_type=f32)
    sigmoid_gate = jax.nn.sigmoid(gate_pre)
    activated = gate_pre * sigmoid_gate
    hidden = (activated * up_pre).astype(bf16)
    grad_gate = (
        grad_hidden * up_pre * sigmoid_gate * (1.0 + gate_pre * (1.0 - sigmoid_gate))
    ).astype(bf16)
    grad_up = (grad_hidden * activated).astype(bf16)
    partial_sum = lax.dot_general(grad_gate, gate, last, preferred_element_type=f32)
    partial_sum += lax.dot_general(grad_up, up, last, preferred_element_type=f32)
    grad_inputs = lax.psum_scatter(partial_sum, "tp", scatter_dimension=1, tiled=True)

    def scattered(lhs, rhs, dimension):
        grads = lax.dot_general(lhs, rhs, first, preferred_element_type=f32)
        grads = lax.psum_scatter(grads, "fs", scatter_dimension=dimension, tiled=True)
        return lax.psum(grads, "rep")

    return (
        grad_inputs.astype(bf16),
        scattered(x, grad_gate, 0),
        scattered(x, grad_up, 0),
        scattered(hidden, c, 1),
    )


def per_device(n_rep, n_fs, n_tp, x, c, gate_weight, up_weight, down_weight):
    n_y = max(k for k in range(1, n_fs + 1) if n_fs % k == 0 and k * k <= n_fs)
    n_z = n_fs // n_y
    tokens, width = x.shape
    depth, hidden_tp = gate_weight.shape
    args = (x, c, gate_weight, up_weight, down_weight)
    whole = hidden_tp % (16 * n_rep * n_z) == 0
    if whole and tokens % 128 == width % 128 == depth % 128 == 0 and min(n_rep, n_y, n_tp) > 1:
        return fused((n_rep, n_fs, n_tp, n_y), *args)
    return gathered(*args)


def solution(mesh):
    n_rep, n_fs, n_tp = (mesh.shape[axis] for axis in ("rep", "fs", "tp"))
    placed = (
        P(("rep", "fs"), "tp"),
        P(("rep", "fs"), "tp"),
        P("fs", "tp"),
        P("fs", "tp"),
        P("tp", "fs"),
    )
    return jax.shard_map(
        functools.partial(per_device, n_rep, n_fs, n_tp),
        mesh=mesh,
        in_specs=placed,
        out_specs=(P(("rep", "fs"), "tp"), P("fs", "tp"), P("fs", "tp"), P("tp", "fs")),
        check_vma=False,
    )
```

```python
import functools

import jax
import jax.numpy as jnp
from jax import lax
from jax.experimental import pallas as pl
from jax.experimental.pallas import tpu as pltpu
from jax.sharding import PartitionSpec as P

MESH = pl.DeviceIdType.MESH


def greet(n_rep, n_fs, n_tp):
    barrier = pltpu.get_barrier_semaphore()
    for axis, n in (("rep", n_rep), ("fs", n_fs), ("tp", n_tp)):
        me = lax.axis_index(axis)
        for k in range(1, n):
            pl.semaphore_signal(
                barrier, inc=1, device_id={axis: lax.rem(me + k, n)}, device_id_type=MESH
            )
    return lambda: pl.semaphore_wait(barrier, n_rep + n_fs + n_tp - 3)


class Sender:
    def __init__(self, sems):
        self.sems, self.used, self.pending = sems, 0, []

    def run(self, build, when):
        if when is None:
            build().start()
        else:
            pl.when(when)(lambda: build().start())

    def send(self, src, dst, recv_sem, axis, peer, when=None):
        def build(at=self.used):
            return pltpu.make_async_remote_copy(
                src_ref=src,
                dst_ref=dst,
                send_sem=self.sems.at[at],
                recv_sem=recv_sem,
                device_id={axis: peer},
                device_id_type=MESH,
            )

        self.used += 1
        self.run(build, when)
        self.pending.append((lambda: build().wait_send(), when))

    def local(self, src, dst):
        def build(at=self.used):
            return pltpu.make_async_copy(src, dst, self.sems.at[at])

        self.used += 1
        self.run(build, None)
        self.pending.append((lambda: build().wait(), None))

    def finish(self):
        for wait, when in self.pending:
            if when is None:
                wait()
            else:
                pl.when(when)(wait)
        self.used, self.pending = 0, []


def arrived(slot, recv_sem, when=None):
    def wait():
        pltpu.make_async_copy(slot, slot, recv_sem).wait()

    if when is None:
        wait()
    else:
        pl.when(when)(wait)


def near_first(n):
    return sorted(range(1, n), key=lambda k: min(k, n - k))


def layer_kernel(
    sizes, *refs
):
    inputs, rest = refs[:5], refs[5:]
    outputs, local, loads, rest = rest[:4], rest[4:9], rest[9], rest[10:]
    met = greet(*sizes[:3])
    copies = [pltpu.make_async_copy(a, b, loads.at[i]) for i, (a, b) in enumerate(zip(inputs, local))]
    for copy in copies:
        copy.start()
    met()
    layer(sizes, copies, *local, *outputs, *rest)


def layer(
    sizes, copies, x_ref, c_ref, gate_ref, up_ref, down_ref, dx_ref, dgate_ref, dup_ref, ddown_ref,
    xa, ca, wt, wa, pre, pre_down, gt, ht, p, p_in, q, x_in, za, za_in, zb, zb_in, xz, xz_in,
    gp, go, g_in, gs, dw,
    sends, act_recv, w_recv, p_recv, x_recv, za_recv, zb_recv, xz_recv, g_recv, d_recv,
):
    n_rep, n_fs, n_tp, n_y = sizes
    n_z = n_fs // n_y
    f32, bf16 = jnp.float32, jnp.bfloat16
    rep, fs, tp = (lax.axis_index(axis) for axis in ("rep", "fs", "tp"))
    z, y = fs // n_y, lax.rem(fs, n_y)
    tokens, width = x_ref.shape
    units, depth = ht.shape[0], down_ref.shape[1]
    early = zb.shape[1]
    late = tokens - early
    out = Sender(sends)

    def span(at, size):
        return pl.ds(pl.multiple_of(at * size, size), size)

    def peers(me, n):
        return [lax.rem(me + k, n) for k in range(1, n)]

    def at_z(other, row=y):
        return other * n_y + row

    far_first, low, high = [], 0, n_z - 1
    for _ in range(n_z):
        above = high - z > z - low
        far_first.append(jnp.where(above, high, low))
        low, high = jnp.where(above, low, low + 1), jnp.where(above, high - 1, high)
    others = far_first[:-1]
    near = [z] + others[::-1]

    own_acts, acts = (x_ref, c_ref), (xa, ca)

    def act_slot(a, shard, part):
        return acts[a].at[span(shard, tokens), span(part, width)]

    def act_send(a, shard, src, axis, peer, when=None):
        out.send(src, act_slot(a, shard, tp), act_recv.at[a, shard, tp], axis, peer, when)

    def to_rep(a, shard, src, when=None):
        for peer in peers(rep, n_rep):
            act_send(a, shard, src, "rep", peer, when)

    def to_tp(a, shard, src, when=None):
        for peer in peers(tp, n_tp):
            act_send(a, shard, src, "tp", peer, when)

    def from_rep(other):
        for peer in peers(rep, n_rep):
            for a in range(2):
                shard = peer * n_z + other
                slot = act_slot(a, shard, tp)
                arrived(slot, act_recv.at[a, shard, tp])
                to_tp(a, shard, slot)

    mine = rep * n_z + z
    for a in range(2):
        copies[a].wait()
        act_send(a, mine, own_acts[a], "fs", fs + n_y, z + 1 < n_z)
        act_send(a, mine, own_acts[a], "fs", fs - n_y, z >= 1)
        to_rep(a, mine, own_acts[a])
    for a in range(2):
        to_tp(a, mine, own_acts[a])

    for copy in copies[2:]:
        copy.wait()
    wt[0] = gate_ref[...].T
    wt[1] = up_ref[...].T

    def w_part(i, owner):
        rows = span(owner, units)
        return down_ref.at[rows] if i == 2 else wt.at[i, rows]

    def w_slot(i, block):
        return wa.at[pl.ds(i * units, units), span(block, depth)]

    def w_send(i, block, src, peer, when=None):
        out.send(src, w_slot(i, block), w_recv.at[i, block], "fs", peer, when)

    for i in range(3):
        for row in peers(y, n_y):
            w_send(i, fs, w_part(i, mine), at_z(z, row))
    for i in range(3):
        wa[i * units : (i + 1) * units, span(fs, depth)] = w_part(i, mine)[...]
    for a in range(2):
        acts[a][span(mine, tokens), span(tp, width)] = own_acts[a][...]

    def send_weights(steps):
        for step in steps:
            for sign, here in ((1, z + step < n_z), (-1, z >= step)):
                other = z + sign * step
                for i in range(3):
                    w_send(i, fs, w_part(i, rep * n_z + other), at_z(other), here)

    def swap_weights(other):
        for i in range(3):
            slot = w_slot(i, at_z(other))
            arrived(slot, w_recv.at[i, at_z(other)])
            for row in peers(y, n_y):
                w_send(i, at_z(other), slot, at_z(z, row))

    swapped = 1
    for k in range(1, n_z):
        for a in range(2):
            for here, onward, step in ((z >= k, z + 1 < n_z, -1), (z + k < n_z, z >= 1, 1)):
                shard = mine + step * k
                slot = act_slot(a, shard, tp)
                arrived(slot, act_recv.at[a, shard, tp], here)
                if k < n_z - 1:
                    act_send(a, shard, slot, "fs", fs - step * n_y, jnp.logical_and(here, onward))
                to_rep(a, shard, slot, here)
                to_tp(a, shard, slot, here)
            if k < n_z - 1:
                continue
            if a == 0:
                send_weights([k])
            if swapped < k:
                swap_weights(near[swapped])
                swapped += 1
        if k < n_z - 1:
            send_weights([k])
        if k == 1:
            from_rep(z)
        if 1 < k == n_z - 2:
            swap_weights(near[1])
            swapped = 2
    if n_z == 1:
        from_rep(z)
    for k in range(swapped, n_z):
        swap_weights(near[k])
    for k in range(1, n_z):
        from_rep(near[k])
    for part in peers(tp, n_tp):
        for shard in range(n_rep * n_z):
            for a in range(2):
                arrived(act_slot(a, shard, part), act_recv.at[a, shard, part])

    last = (((1,), (1,)), ((), ()))
    first = (((0,), (0,)), ((), ()))

    def contract(block, fresh):
        cols = span(block, depth)
        for ref, rows, act in ((pre, slice(0, 2 * units), xa), (pre_down, slice(2 * units, 3 * units), ca)):
            part = lax.dot_general(wa[rows, cols], act[:, cols], last, preferred_element_type=f32)
            ref[...] = part if fresh else ref[...] + part

    for k in range(n_z):
        contract(at_z(near[k]), k == 0)
        for row in peers(y, n_y):
            for i in range(3):
                arrived(w_slot(i, at_z(near[k], row)), w_recv.at[i, at_z(near[k], row)])
            contract(at_z(near[k], row), False)

    out.finish()

    def activate(side):
        cols = span(side, n_z * tokens)

        @pl.loop(0, units // 16)
        def _(step):
            rows, more = span(step, 16), pl.ds(pl.multiple_of(units + step * 16, 16), 16)
            gate_pre, up_pre, grad_hidden = pre[rows, cols], pre[more, cols], pre_down[rows, cols]
            sigmoid_gate = jax.nn.sigmoid(gate_pre)
            activated = gate_pre * sigmoid_gate
            ht[rows, cols] = (activated * up_pre).astype(bf16)
            gt[rows, cols] = (
                grad_hidden * up_pre * sigmoid_gate * (1.0 + gate_pre * (1.0 - sigmoid_gate))
            ).astype(bf16)
            gt[more, cols] = (grad_hidden * activated).astype(bf16)

    def partial_inputs(side):
        rows = span(side, n_z * tokens)
        p[rows] = lax.dot_general(
            gt[:, rows], wa[: 2 * units], first, preferred_element_type=f32
        ).astype(bf16)
        for other in far_first:
            shard = side * n_z + other
            for j in range(1, n_tp):
                peer = lax.rem(tp + j, n_tp)
                out.send(
                    p.at[span(shard, tokens), span(peer, width)],
                    p_in.at[j - 1, shard],
                    p_recv.at[j - 1, shard],
                    "tp",
                    peer,
                )

    def pair_wait(shard):
        for j in range(n_tp - 1):
            arrived(p_in.at[j, shard], p_recv.at[j, shard])

    def pair_sum(shard, low, size):
        rows = pl.ds(pl.multiple_of(shard * tokens + low, 16), size)
        total = p[rows, span(tp, width)].astype(f32)
        for j in range(n_tp - 1):
            total = total + p_in[j, shard, low : low + size].astype(f32)
        return total

    def weight_block(block, dst):
        cols = span(block, depth)
        dst[: 2 * units] = jnp.dot(gt[...], xa[:, cols], preferred_element_type=f32).astype(
            dst.dtype
        )
        dst[2 * units :] = jnp.dot(ht[...], ca[:, cols], preferred_element_type=f32).astype(
            dst.dtype
        )

    def chain(value, buf, box, box_recv, other, inner):
        up = other > z
        came = jnp.where(up, 0, 1)
        behind = jnp.where(up, z >= 1, z + 1 < n_z)

        @pl.when(behind if inner else jnp.logical_not(behind))
        def _():
            for low, size, total in value(other):
                rows = pl.ds(low, size)
                if inner:
                    if low == 0:
                        arrived(box.at[came, other], box_recv.at[came, other])
                    total = total + box[came, other, rows].astype(f32)
                buf[other, rows] = total.astype(bf16)

        if inner:
            out.send(
                buf.at[other], box.at[came, other], box_recv.at[came, other],
                "fs", jnp.where(up, fs + n_y, fs - n_y), behind,
            )
        else:
            out.send(
                buf.at[other], box.at[came, other], box_recv.at[came, other],
                "fs", jnp.where(up, fs + n_y, fs - n_y), jnp.logical_not(behind),
            )

    def chain_end(value, acc, box, box_recv):
        for low, size, total in value(z):
            acc[pl.ds(low, size)] = total
        for came, here in ((0, z >= 1), (1, z + 1 < n_z)):

            @pl.when(here)
            def _():
                arrived(box.at[came, z], box_recv.at[came, z])
                acc[...] = acc[...] + box[came, z].astype(f32)

    def late_rows(other):
        return [
            (side * late, late, pair_sum(side * n_z + other, early, late)) for side in range(n_rep)
        ]

    def early_rows(other):
        total = pair_sum(rep * n_z + other, 0, early)
        for j in range(n_rep - 1):
            total = total + x_in[j, other].astype(f32)
        return [(0, early, total)]

    def x_arrived(other):
        for j in range(n_rep - 1):
            arrived(x_in.at[j, other], x_recv.at[j, other])

    def dw_slot(side, other):
        return dw.at[side * n_z + other]

    def dw_send(other, src):
        for peer in peers(rep, n_rep):
            out.send(src, dw_slot(rep, other), d_recv.at[rep, other], "rep", peer)

    def g_step(other, mine_too):
        total = go[other]
        for j in range(n_y - 1):
            arrived(g_in.at[j, other], g_recv.at[j, other])
            total = total + g_in[j, other].astype(f32)
        if mine_too:
            dw[mine] = total.astype(bf16)
            dw_send(z, dw_slot(rep, z))
        else:
            gs[other] = total.astype(bf16)
            out.send(gs.at[other], dw_slot(rep, z), d_recv.at[rep, z], "fs", at_z(other))

    def g_forward(other):
        arrived(dw_slot(rep, other), d_recv.at[rep, other])
        dw_send(other, dw_slot(rep, other))

    def to_row(other):
        for j in range(1, n_y):
            row = lax.rem(y + j, n_y)
            weight_block(at_z(other, row), gp.at[j - 1, other])
            out.send(
                gp.at[j - 1, other], g_in.at[j - 1, other], g_recv.at[j - 1, other],
                "fs", at_z(z, row),
            )

    def to_side(other):
        for j in range(1, n_rep):
            side = lax.rem(rep + j, n_rep)
            pair_wait(side * n_z + other)
            q[j - 1, other] = pair_sum(side * n_z + other, 0, early).astype(bf16)
            out.send(
                q.at[j - 1, other], x_in.at[j - 1, other], x_recv.at[j - 1, other], "rep", side
            )

    for j in range(1, n_rep):
        side = lax.rem(rep + j, n_rep)
        activate(side)
        partial_inputs(side)
    activate(rep)
    to_row(z)
    for other in far_first:
        to_side(other)
    partial_inputs(rep)
    for other in others:
        to_row(other)
    for other in far_first:
        pair_wait(rep * n_z + other)
    for other in others:
        chain(late_rows, za, za_in, za_recv, other, False)
    for other in [z] + others:
        weight_block(at_z(other), go.at[other])
    def late_on(other):
        chain(late_rows, za, za_in, za_recv, other, True)

    g_step(z, True)
    for i, other in enumerate(others):
        g_step(other, False)
        x_arrived(other)
        chain(early_rows, zb, zb_in, zb_recv, other, False)
        if i:
            late_on(others[i - 1])
    if others:
        late_on(others[-1])
    chain_end(late_rows, xz.at[0, : n_rep * late], za_in, za_recv)
    for j in range(1, n_rep):
        side = lax.rem(rep + j, n_rep)
        xz_in[j - 1, 0] = xz[0, span(side, late)].astype(bf16)
        out.send(xz_in.at[j - 1, 0], xz_in.at[j - 1, 1], xz_recv.at[j - 1], "rep", side)
    for other in others:
        g_forward(other)
        chain(early_rows, zb, zb_in, zb_recv, other, True)
    x_arrived(z)
    chain_end(early_rows, xz.at[1, :early], zb_in, zb_recv)
    dx_ref[:early] = xz[1, :early].astype(bf16)
    total = xz[0, span(rep, late)]
    for j in range(n_rep - 1):
        arrived(xz_in.at[j, 1], xz_recv.at[j])
        total = total + xz_in[j, 1].astype(f32)
    dx_ref[early:] = total.astype(bf16)
    for side in peers(rep, n_rep):
        for other in [z] + others:
            arrived(dw_slot(side, other), d_recv.at[side, other])
    whole = dw[...]
    dgate_ref[...] = whole[:, :units].reshape(dgate_ref.shape[::-1]).T
    dup_ref[...] = whole[:, units : 2 * units].reshape(dup_ref.shape[::-1]).T
    ddown_ref[...] = whole[:, 2 * units :].reshape(ddown_ref.shape)
    out.finish()


VMEM = pl.BlockSpec(memory_space=pltpu.VMEM)
ANY = pl.BlockSpec(memory_space=pl.ANY)
DMA = pltpu.SemaphoreType.DMA


def fused(sizes, x, c, gate_weight, up_weight, down_weight):
    bf16, f32 = jnp.bfloat16, jnp.float32
    n_rep, n_fs, n_tp, n_y = sizes
    n_z = n_fs // n_y
    tokens, width = x.shape
    depth, hidden_tp = gate_weight.shape
    model, units = width * n_tp, hidden_tp // (n_rep * n_z)
    shards = n_rep * n_z
    group = shards * tokens
    tp_rep = n_tp + n_rep - 2
    n_sends = (
        2 * (2 + tp_rep) + 4 * ((n_z - 1) * (1 + tp_rep) - 1) + 2 * n_z * (n_rep - 1) * (n_tp - 1)
        + 3 * (n_y - 1) * n_z + 6 * (n_z - 1)
    )
    late = tokens * 3 // 128 * 16
    early = tokens - late
    grad_inputs, *grads = pl.pallas_call(
        functools.partial(layer_kernel, sizes),
        out_shape=(
            jax.ShapeDtypeStruct((tokens, width), bf16),
            jax.ShapeDtypeStruct((depth, hidden_tp), bf16),
            jax.ShapeDtypeStruct((depth, hidden_tp), bf16),
            jax.ShapeDtypeStruct((hidden_tp, depth), bf16),
        ),
        in_specs=[ANY] * 5,
        out_specs=(VMEM,) * 4,
        scratch_shapes=[
            *(pltpu.VMEM(v.shape, bf16) for v in (x, c, gate_weight, up_weight, down_weight)),
            DMA((5,)),
            pltpu.VMEM((group, model), bf16),
            pltpu.VMEM((group, model), bf16),
            pltpu.VMEM((2, hidden_tp, depth), bf16),
            pltpu.VMEM((3 * units, model), bf16),
            pltpu.VMEM((2 * units, group), f32),
            pltpu.VMEM((units, group), f32),
            pltpu.VMEM((2 * units, group), bf16),
            pltpu.VMEM((units, group), bf16),
            pltpu.VMEM((group, model), bf16),
            pltpu.VMEM((n_tp - 1, shards, tokens, width), bf16),
            pltpu.VMEM((n_rep - 1, n_z, early, width), bf16),
            pltpu.VMEM((n_rep - 1, n_z, early, width), bf16),
            pltpu.VMEM((n_z, n_rep * late, width), bf16),
            pltpu.VMEM((2, n_z, n_rep * late, width), bf16),
            pltpu.VMEM((n_z, early, width), bf16),
            pltpu.VMEM((2, n_z, early, width), bf16),
            pltpu.VMEM((2, max(early, n_rep * late), width), f32),
            pltpu.VMEM((n_rep - 1, 2, late, width), bf16),
            pltpu.VMEM((n_y - 1, n_z, 3 * units, depth), bf16),
            pltpu.VMEM((n_z, 3 * units, depth), f32),
            pltpu.VMEM((n_y - 1, n_z, 3 * units, depth), bf16),
            pltpu.VMEM((n_z, 3 * units, depth), bf16),
            pltpu.VMEM((shards, 3 * units, depth), bf16),
            DMA((n_sends,)),
            DMA((2, shards, n_tp)),
            DMA((3, n_fs)),
            DMA((n_tp - 1, shards)),
            DMA((n_rep - 1, n_z)),
            DMA((2, n_z)),
            DMA((2, n_z)),
            DMA((n_rep - 1,)),
            DMA((n_y - 1, n_z)),
            DMA((n_rep, n_z)),
        ],
        compiler_params=pltpu.CompilerParams(
            collective_id=0, has_side_effects=True, vmem_limit_bytes=60 * 2**20
        ),
    )(x, c, gate_weight, up_weight, down_weight)
    return grad_inputs, *(v.astype(f32) for v in grads)


def gathered(x, c, gate_weight, up_weight, down_weight):
    bf16, f32 = jnp.bfloat16, jnp.float32
    last = (((1,), (1,)), ((), ()))
    first = (((0,), (0,)), ((), ()))
    x, c = (lax.all_gather(v, "tp", axis=1, tiled=True) for v in (x, c))
    gate, up = (lax.all_gather(v, "fs", axis=0, tiled=True) for v in (gate_weight, up_weight))
    down = lax.all_gather(down_weight, "fs", axis=1, tiled=True)
    gate_pre = jnp.dot(x, gate, preferred_element_type=f32)
    up_pre = jnp.dot(x, up, preferred_element_type=f32)
    grad_hidden = lax.dot_general(c, down, last, preferred_element_type=f32)
    sigmoid_gate = jax.nn.sigmoid(gate_pre)
    activated = gate_pre * sigmoid_gate
    hidden = (activated * up_pre).astype(bf16)
    grad_gate = (
        grad_hidden * up_pre * sigmoid_gate * (1.0 + gate_pre * (1.0 - sigmoid_gate))
    ).astype(bf16)
    grad_up = (grad_hidden * activated).astype(bf16)
    partial_sum = lax.dot_general(grad_gate, gate, last, preferred_element_type=f32)
    partial_sum += lax.dot_general(grad_up, up, last, preferred_element_type=f32)
    grad_inputs = lax.psum_scatter(partial_sum, "tp", scatter_dimension=1, tiled=True)

    def scattered(lhs, rhs, dimension):
        grads = lax.dot_general(lhs, rhs, first, preferred_element_type=f32)
        grads = lax.psum_scatter(grads, "fs", scatter_dimension=dimension, tiled=True)
        return lax.psum(grads, "rep")

    return (
        grad_inputs.astype(bf16),
        scattered(x, grad_gate, 0),
        scattered(x, grad_up, 0),
        scattered(hidden, c, 1),
    )


def per_device(n_rep, n_fs, n_tp, x, c, gate_weight, up_weight, down_weight):
    n_y = max(k for k in range(1, n_fs + 1) if n_fs % k == 0 and k * k <= n_fs)
    n_z = n_fs // n_y
    tokens, width = x.shape
    depth, hidden_tp = gate_weight.shape
    args = (x, c, gate_weight, up_weight, down_weight)
    whole = hidden_tp % (16 * n_rep * n_z) == 0
    if whole and tokens % 128 == width % 128 == depth % 128 == 0 and min(n_rep, n_y, n_tp) > 1:
        return fused((n_rep, n_fs, n_tp, n_y), *args)
    return gathered(*args)


def solution(mesh):
    n_rep, n_fs, n_tp = (mesh.shape[axis] for axis in ("rep", "fs", "tp"))
    placed = (
        P(("rep", "fs"), "tp"),
        P(("rep", "fs"), "tp"),
        P("fs", "tp"),
        P("fs", "tp"),
        P("tp", "fs"),
    )
    return jax.shard_map(
        functools.partial(per_device, n_rep, n_fs, n_tp),
        mesh=mesh,
        in_specs=placed,
        out_specs=(P(("rep", "fs"), "tp"), P("fs", "tp"), P("fs", "tp"), P("tp", "fs")),
        check_vma=False,
    )
```

```python
import functools

import jax
import jax.numpy as jnp
from jax import lax
from jax.experimental import pallas as pl
from jax.experimental.pallas import tpu as pltpu
from jax.sharding import PartitionSpec as P

MESH = pl.DeviceIdType.MESH


def greet(n_rep, n_fs, n_tp):
    barrier = pltpu.get_barrier_semaphore()
    for axis, n in (("rep", n_rep), ("fs", n_fs), ("tp", n_tp)):
        me = lax.axis_index(axis)
        for k in range(1, n):
            pl.semaphore_signal(
                barrier, inc=1, device_id={axis: lax.rem(me + k, n)}, device_id_type=MESH
            )
    return lambda: pl.semaphore_wait(barrier, n_rep + n_fs + n_tp - 3)


class Sender:
    def __init__(self, sems):
        self.sems, self.used, self.pending = sems, 0, []

    def run(self, build, when):
        if when is None:
            build().start()
        else:
            pl.when(when)(lambda: build().start())

    def send(self, src, dst, recv_sem, axis, peer, when=None):
        def build(at=self.used):
            return pltpu.make_async_remote_copy(
                src_ref=src,
                dst_ref=dst,
                send_sem=self.sems.at[at],
                recv_sem=recv_sem,
                device_id={axis: peer},
                device_id_type=MESH,
            )

        self.used += 1
        self.run(build, when)
        self.pending.append((lambda: build().wait_send(), when))

    def local(self, src, dst):
        def build(at=self.used):
            return pltpu.make_async_copy(src, dst, self.sems.at[at])

        self.used += 1
        self.run(build, None)
        self.pending.append((lambda: build().wait(), None))

    def finish(self):
        for wait, when in self.pending:
            if when is None:
                wait()
            else:
                pl.when(when)(wait)
        self.used, self.pending = 0, []


def arrived(slot, recv_sem, when=None):
    def wait():
        pltpu.make_async_copy(slot, slot, recv_sem).wait()

    if when is None:
        wait()
    else:
        pl.when(when)(wait)


def near_first(n):
    return sorted(range(1, n), key=lambda k: min(k, n - k))


def layer_kernel(
    sizes, *refs
):
    inputs, rest = refs[:5], refs[5:]
    outputs, local, loads, rest = rest[:4], rest[4:9], rest[9], rest[10:]
    met = greet(*sizes[:3])
    copies = [pltpu.make_async_copy(a, b, loads.at[i]) for i, (a, b) in enumerate(zip(inputs, local))]
    for copy in copies:
        copy.start()
    met()
    layer(sizes, copies, *local, *outputs, *rest)


def layer(
    sizes, copies, x_ref, c_ref, gate_ref, up_ref, down_ref, dx_ref, dgate_ref, dup_ref, ddown_ref,
    xa, ca, wt, wa, wa_more, pre, pre_down, gt, ht,
    p, p_in, q, x_in, r, z_in, total,
    gp, go, g_in, gs, dw, gp_more, go_more, g_in_more, gs_more, dw_more,
    sends, act_recv, w_recv, p_recv, x_recv, z_recv, g_recv, d_recv,
):
    n_rep, n_fs, n_tp, n_y = sizes
    n_z = n_fs // n_y
    f32, bf16 = jnp.float32, jnp.bfloat16
    rep, fs, tp = (lax.axis_index(axis) for axis in ("rep", "fs", "tp"))
    z, y = fs // n_y, lax.rem(fs, n_y)
    tokens, width = x_ref.shape
    base, more, depth = wa.shape[1], ht.shape[0] - wa.shape[1], down_ref.shape[1]
    units = base + more
    inner = jnp.logical_and(z > 0, z < n_z - 1) if more else None
    out = Sender(sends)

    def span(at, size):
        return pl.ds(pl.multiple_of(at * size, size), size)

    def peers(me, n):
        return [lax.rem(me + k, n) for k in range(1, n)]

    def at_z(other, row=y):
        return other * n_y + row

    far_first, low, high = [], 0, n_z - 1
    for _ in range(n_z):
        above = 2 * (high - z) + jnp.where(2 * z < n_z, 1, 0) > 2 * (z - low)
        far_first.append(jnp.where(above, high, low))
        low, high = jnp.where(above, low, low + 1), jnp.where(above, high - 1, high)
    others = far_first[:-1]
    near = [z] + others[::-1]

    own_acts, acts = (x_ref, c_ref), (xa, ca)

    def act_slot(a, shard, part):
        return acts[a].at[span(shard, tokens), span(part, width)]

    def act_send(a, shard, src, axis, peer, when=None):
        out.send(src, act_slot(a, shard, tp), act_recv.at[a, shard, tp], axis, peer, when)

    def to_rep(a, shard, src, when=None):
        for peer in peers(rep, n_rep):
            act_send(a, shard, src, "rep", peer, when)

    def to_tp(a, shard, src, when=None):
        for peer in peers(tp, n_tp):
            act_send(a, shard, src, "tp", peer, when)

    def from_rep(other):
        for peer in peers(rep, n_rep):
            for a in range(2):
                shard = peer * n_z + other
                slot = act_slot(a, shard, tp)
                arrived(slot, act_recv.at[a, shard, tp])
                to_tp(a, shard, slot)

    mine = rep * n_z + z
    for a in range(2):
        copies[a].wait()
        act_send(a, mine, own_acts[a], "fs", fs + n_y, z + 1 < n_z)
        act_send(a, mine, own_acts[a], "fs", fs - n_y, z >= 1)
        to_rep(a, mine, own_acts[a])
    for a in range(2):
        to_tp(a, mine, own_acts[a])

    for copy in copies[2:]:
        copy.wait()
    wt[0] = gate_ref[...].T
    wt[1] = up_ref[...].T

    def inside(other):
        return jnp.logical_and(other > 0, other < n_z - 1)

    parts = [(0, 0), (0, 1), (1, 0), (1, 1)][: 4 if more else 2]
    here_too = {0: None, 1: inner}

    def w_part(extra, kind, other):
        start = rep * (n_z * base + max(n_z - 2, 0) * more) + other * units
        start = start - (jnp.minimum(other, 1) * more if more else 0) + extra * base
        rows = pl.ds(pl.multiple_of(start, 16), more if extra else base)
        return down_ref.at[rows] if kind else wt.at[:, rows]

    def w_slot(extra, kind, block):
        held = wa_more if extra else wa
        return held.at[2 if kind else slice(0, 2), :, span(block, depth)]

    def w_send(part, block, src, peer, when=None):
        out.send(src, w_slot(*part, block), w_recv.at[parts.index(part), block], "fs", peer, when)

    def w_arrived(part, block):
        arrived(w_slot(*part, block), w_recv.at[parts.index(part), block], here_too[part[0]])

    for part in parts:
        for row in peers(y, n_y):
            w_send(part, fs, w_part(*part, z), at_z(z, row), here_too[part[0]])

    def keep(part):
        held, (extra, kind) = (wa_more if part[0] else wa), part
        if kind:
            held[2, :, span(fs, depth)] = w_part(*part, z)[...]
        else:
            held[0:2, :, span(fs, depth)] = w_part(*part, z)[...]

    for part in parts:
        if part[0]:
            pl.when(inner)(functools.partial(keep, part))
        else:
            keep(part)
    for a in range(2):
        acts[a][span(mine, tokens), span(tp, width)] = own_acts[a][...]

    def send_weights(step, only=None):
        for sign, here in ((1, z + step < n_z), (-1, z >= step)):
            other = z + sign * step
            here = here if only is None else jnp.logical_and(here, only)
            for part in parts:
                when = jnp.logical_and(here, inside(other)) if part[0] else here
                w_send(part, fs, w_part(*part, other), at_z(other), when)

    def swap_weights(other):
        for part in parts:
            block = at_z(other)
            w_arrived(part, block)
            for row in peers(y, n_y):
                w_send(part, block, w_slot(*part, block), at_z(z, row), here_too[part[0]])

    held = n_z > 3
    for k in range(1, n_z):
        for a in range(2):
            for here, onward, step in ((z >= k, z + 1 < n_z, -1), (z + k < n_z, z >= 1, 1)):
                shard = mine + step * k
                slot = act_slot(a, shard, tp)
                arrived(slot, act_recv.at[a, shard, tp], here)
                if k < n_z - 1:
                    act_send(a, shard, slot, "fs", fs - step * n_y, jnp.logical_and(here, onward))
                to_rep(a, shard, slot, here)
                to_tp(a, shard, slot, here)
            if k == n_z - 1 and a == 0:
                send_weights(k)
        if k < n_z - 2 or not held and k == n_z - 2:
            send_weights(k)
        if k == 1:
            from_rep(z)
        if held and k == n_z - 2:
            send_weights(k, jnp.logical_not(inside(z)))
            swap_weights(near[1])
    if n_z == 1:
        from_rep(z)
    if held:
        swap_weights(near[2])
        send_weights(n_z - 2, inside(z))
    for k in range(3 if held else 1, n_z):
        swap_weights(near[k])
    for k in range(1, n_z):
        from_rep(near[k])
    for part in peers(tp, n_tp):
        for shard in range(n_rep * n_z):
            for a in range(2):
                arrived(act_slot(a, shard, part), act_recv.at[a, shard, part])

    last = (((1,), (1,)), ((), ()))
    first = (((0,), (0,)), ((), ()))

    def by_place(work):
        if not more:
            work(False)
        else:
            pl.when(inner)(lambda: work(True))
            pl.when(jnp.logical_not(inner))(lambda: work(False))

    def weights(full, kind, cols):
        rows = slice(2, 3) if kind else slice(0, 2)
        value = wa[rows, :, cols]
        value = value.reshape(-1, value.shape[-1])
        if full:
            extra = wa_more[rows, :, cols]
            value = jnp.concatenate([value, extra.reshape(-1, value.shape[-1])], axis=0)
        return value

    def contract(block, fresh):
        cols = span(block, depth)

        def work(full):
            for kind, ref, act in ((0, pre, xa), (1, pre_down, ca)):
                lhs = weights(full, kind, cols)
                part = lax.dot_general(lhs, act[:, cols], last, preferred_element_type=f32)
                rows = slice(0, lhs.shape[0])
                ref[rows] = part if fresh else ref[rows] + part

        by_place(work)

    for k in range(n_z):
        contract(at_z(near[k]), k == 0)
        for row in peers(y, n_y):
            for part in parts:
                w_arrived(part, at_z(near[k], row))
            contract(at_z(near[k], row), False)
    out.finish()

    def activate(side):
        cols = span(side, n_z * tokens)

        def rows_of(start, size, down):
            @pl.loop(0, size // 16)
            def _(step):
                gate = pl.ds(pl.multiple_of(start + step * 16, 16), 16)
                up = pl.ds(pl.multiple_of(start + size + step * 16, 16), 16)
                rows = pl.ds(pl.multiple_of(down + step * 16, 16), 16)
                gate_pre, up_pre, grad_hidden = pre[gate, cols], pre[up, cols], pre_down[rows, cols]
                sigmoid_gate = jax.nn.sigmoid(gate_pre)
                activated = gate_pre * sigmoid_gate
                ht[rows, cols] = (activated * up_pre).astype(bf16)
                gt[gate, cols] = (
                    grad_hidden * up_pre * sigmoid_gate * (1.0 + gate_pre * (1.0 - sigmoid_gate))
                ).astype(bf16)
                gt[up, cols] = (grad_hidden * activated).astype(bf16)

        rows_of(0, base, 0)
        if more:
            pl.when(inner)(lambda: rows_of(2 * base, more, base))

    def partial_inputs(side):
        rows = span(side, n_z * tokens)

        def work(full):
            rhs = weights(full, 0, slice(None))
            p[rows] = lax.dot_general(
                gt[: rhs.shape[0], rows], rhs, first, preferred_element_type=f32
            ).astype(bf16)

        by_place(work)
        for other in far_first:
            shard = side * n_z + other
            for j in range(1, n_tp):
                peer = lax.rem(tp + j, n_tp)
                out.send(
                    p.at[span(shard, tokens), span(peer, width)],
                    p_in.at[j - 1, shard],
                    p_recv.at[j - 1, shard],
                    "tp",
                    peer,
                )

    def pair_wait(shard):
        for j in range(n_tp - 1):
            arrived(p_in.at[j, shard], p_recv.at[j, shard])

    def pair_sum(shard):
        value = p[span(shard, tokens), span(tp, width)].astype(f32)
        for j in range(n_tp - 1):
            value = value + p_in[j, shard].astype(f32)
        return value

    def weight_block(block, dst, dst_more):
        cols = span(block, depth)

        def work(full):
            held = units if full else base
            both = jnp.dot(gt[: 2 * held], xa[:, cols], preferred_element_type=f32)
            down = jnp.dot(ht[:held], ca[:, cols], preferred_element_type=f32)
            dst[: 2 * base] = both[: 2 * base].astype(dst.dtype)
            dst[2 * base :] = down[:base].astype(dst.dtype)
            if full:
                dst_more[: 2 * more] = both[2 * base :].astype(dst.dtype)
                dst_more[2 * more :] = down[base:].astype(dst.dtype)

        by_place(work)

    def rep_sum(other):
        value = pair_sum(rep * n_z + other)
        for j in range(n_rep - 1):
            value = value + x_in[j, other].astype(f32)
        return value

    def rep_wait(other):
        for j in range(n_rep - 1):
            arrived(x_in.at[j, other], x_recv.at[j, other])

    def toward(other, passing):
        up = other > z
        came = jnp.where(up, 0, 1)
        behind = jnp.where(up, z >= 1, z + 1 < n_z)
        when = behind if passing else jnp.logical_not(behind)
        slot, recv_sem = z_in.at[came, other], z_recv.at[came, other]

        @pl.when(when)
        def _():
            rep_wait(other)
            value = rep_sum(other)
            if passing:
                arrived(slot, recv_sem)
                value = value + slot[...].astype(f32)
            r[other] = value.astype(bf16)

        peer = jnp.where(up, fs + n_y, fs - n_y)
        out.send(r.at[other], slot, recv_sem, "fs", peer, when)

    sets = [(gp, go, g_in, gs, dw)]
    if more:
        sets.append((gp_more, go_more, g_in_more, gs_more, dw_more))

    def dw_slot(extra, side, other):
        if extra:
            other = jnp.clip(other - 1, 0, n_z - 3)
            return dw_more.at[side * (n_z - 2) + other]
        return dw.at[side * n_z + other]

    def dw_send(extra, other, when):
        slot = dw_slot(extra, rep, other)
        for peer in peers(rep, n_rep):
            out.send(slot, slot, d_recv.at[extra, rep, other], "rep", peer, when)

    def g_step(other, own):
        def work(extra):
            partial, total, came, summed, _ = sets[extra]
            total = total[other]
            for j in range(n_y - 1):
                arrived(came.at[j, other], g_recv.at[extra, j, other])
                total = total + came[j, other].astype(f32)
            if own:
                dw_slot(extra, rep, z)[...] = total.astype(bf16)
            else:
                summed[other] = total.astype(bf16)

        for extra in range(len(sets)):
            if extra:
                pl.when(inner)(lambda: work(1))
            else:
                work(0)
            if own:
                dw_send(extra, z, here_too[extra])
            else:
                out.send(
                    sets[extra][3].at[other], dw_slot(extra, rep, z), d_recv.at[extra, rep, z],
                    "fs", at_z(other), here_too[extra],
                )

    def g_forward(other):
        for extra in range(len(sets)):
            when = inside(other) if extra else None
            arrived(dw_slot(extra, rep, other), d_recv.at[extra, rep, other], when)
            dw_send(extra, other, when)

    def to_row(other):
        for j in range(1, n_y):
            row = lax.rem(y + j, n_y)
            at = (j - 1, other)
            weight_block(at_z(other, row), gp.at[at], gp_more.at[at])
            for extra, (partial, _, came, *_) in enumerate(sets):
                out.send(
                    partial.at[at], came.at[at], g_recv.at[extra, j - 1, other],
                    "fs", at_z(z, row), here_too[extra],
                )

    def to_side(other):
        for j in range(1, n_rep):
            side = lax.rem(rep + j, n_rep)
            pair_wait(side * n_z + other)
            q[j - 1, other] = pair_sum(side * n_z + other).astype(bf16)
            out.send(
                q.at[j - 1, other], x_in.at[j - 1, other], x_recv.at[j - 1, other], "rep", side
            )

    for j in range(1, n_rep):
        side = lax.rem(rep + j, n_rep)
        activate(side)
        partial_inputs(side)
    activate(rep)
    rows = others[:-1] + [z] + others[-1:]
    to_row(rows[0])
    for other in far_first:
        to_side(other)
    for other in rows[1:]:
        to_row(other)
    partial_inputs(rep)
    for other in rows:
        weight_block(at_z(other), go.at[other], go_more.at[other])
    for other in far_first:
        pair_wait(rep * n_z + other)

    for other in others[:1]:
        toward(other, False)
    for other in others[:-1]:
        g_step(other, False)
    for other in others[:1]:
        toward(other, True)
    g_step(z, True)
    for other in others[1:2]:
        g_forward(other)
        toward(other, False)
    for other in others[-1:]:
        g_step(other, False)
    for other in others[2:]:
        toward(other, False)
    for other in others[:1]:
        g_forward(other)
    for other in others[1:][-1:]:
        toward(other, True)
    for other in others[2:]:
        g_forward(other)
    for other in others[1:-1]:
        toward(other, True)
    rep_wait(z)
    total[...] = rep_sum(z)
    for came, here in ((0, z >= 1), (1, z + 1 < n_z)):

        @pl.when(here)
        def _(came=came):
            arrived(z_in.at[came, z], z_recv.at[came, z])
            total[...] = total[...] + z_in[came, z].astype(f32)

    dx_ref[...] = total[...].astype(bf16)
    for side in peers(rep, n_rep):
        for other in [z] + others:
            for extra in range(len(sets)):
                arrived(
                    dw_slot(extra, side, other), d_recv.at[extra, side, other],
                    inside(other) if extra else None,
                )

    def gathered_rows(kind):
        rows = []
        for side in range(n_rep):
            for other in range(n_z):
                rows.append(dw[side * n_z + other, kind * base : (kind + 1) * base])
                if more and 0 < other < n_z - 1:
                    at = side * (n_z - 2) + other - 1
                    rows.append(dw_more[at, kind * more : (kind + 1) * more])
        return jnp.concatenate(rows, axis=0)

    dgate_ref[...] = gathered_rows(0).T
    dup_ref[...] = gathered_rows(1).T
    ddown_ref[...] = gathered_rows(2)
    out.finish()


VMEM = pl.BlockSpec(memory_space=pltpu.VMEM)
ANY = pl.BlockSpec(memory_space=pl.ANY)
DMA = pltpu.SemaphoreType.DMA


def fused(sizes, x, c, gate_weight, up_weight, down_weight):
    bf16, f32 = jnp.bfloat16, jnp.float32
    n_rep, n_fs, n_tp, n_y = sizes
    n_z = n_fs // n_y
    tokens, width = x.shape
    depth, hidden_tp = gate_weight.shape
    model, per_rep = width * n_tp, hidden_tp // n_rep
    base, more = per_rep // n_z, 0
    for size in range(16, per_rep, 16) if n_z > 2 else ():
        rest = per_rep - (n_z - 2) * size
        if rest % (16 * n_z) == 0 and 4 * size * n_z <= 3 * rest:
            base, more = rest // n_z, size
    units, spare, mids = base + more, max(more, 16), max(n_z - 2, 1)
    kinds = 4 if more else 2
    shards = n_rep * n_z
    group = shards * tokens
    tp_rep = n_tp + n_rep - 2
    n_sends = (
        2 * (2 + tp_rep) + 4 * ((n_z - 1) * (1 + tp_rep) - 1) + 2 * n_z * (n_rep - 1) * (n_tp - 1)
        + kinds * (n_y - 1) * n_z + 2 * kinds * (n_z - 1 + (n_z > 3))
    )
    grad_inputs, *grads = pl.pallas_call(
        functools.partial(layer_kernel, sizes),
        out_shape=(
            jax.ShapeDtypeStruct((tokens, width), bf16),
            jax.ShapeDtypeStruct((depth, hidden_tp), bf16),
            jax.ShapeDtypeStruct((depth, hidden_tp), bf16),
            jax.ShapeDtypeStruct((hidden_tp, depth), bf16),
        ),
        in_specs=[ANY] * 5,
        out_specs=(VMEM,) * 4,
        scratch_shapes=[
            *(pltpu.VMEM(v.shape, bf16) for v in (x, c, gate_weight, up_weight, down_weight)),
            DMA((5,)),
            pltpu.VMEM((group, model), bf16),
            pltpu.VMEM((group, model), bf16),
            pltpu.VMEM((2, hidden_tp, depth), bf16),
            pltpu.VMEM((3, base, model), bf16),
            pltpu.VMEM((3, spare, model), bf16),
            pltpu.VMEM((2 * units, group), f32),
            pltpu.VMEM((units, group), f32),
            pltpu.VMEM((2 * units, group), bf16),
            pltpu.VMEM((units, group), bf16),
            pltpu.VMEM((group, model), bf16),
            pltpu.VMEM((n_tp - 1, shards, tokens, width), bf16),
            pltpu.VMEM((n_rep - 1, n_z, tokens, width), bf16),
            pltpu.VMEM((n_rep - 1, n_z, tokens, width), bf16),
            pltpu.VMEM((n_z, tokens, width), bf16),
            pltpu.VMEM((2, n_z, tokens, width), bf16),
            pltpu.VMEM((tokens, width), f32),
            *(
                pltpu.VMEM((*lead, 3 * size, depth), kind)
                for size, places in ((base, shards), (spare, n_rep * mids))
                for lead, kind in (
                    ((n_y - 1, n_z), bf16), ((n_z,), f32), ((n_y - 1, n_z), bf16),
                    ((n_z,), bf16), ((places,), bf16),
                )
            ),
            DMA((n_sends,)),
            DMA((2, shards, n_tp)),
            DMA((kinds, n_fs)),
            DMA((n_tp - 1, shards)),
            DMA((n_rep - 1, n_z)),
            DMA((2, n_z)),
            DMA((kinds // 2, n_y - 1, n_z)),
            DMA((kinds // 2, n_rep, n_z)),
        ],
        compiler_params=pltpu.CompilerParams(
            collective_id=0, has_side_effects=True, vmem_limit_bytes=60 * 2**20
        ),
    )(x, c, gate_weight, up_weight, down_weight)
    return grad_inputs, *(v.astype(f32) for v in grads)


def gathered(x, c, gate_weight, up_weight, down_weight):
    bf16, f32 = jnp.bfloat16, jnp.float32
    last = (((1,), (1,)), ((), ()))
    first = (((0,), (0,)), ((), ()))
    x, c = (lax.all_gather(v, "tp", axis=1, tiled=True) for v in (x, c))
    gate, up = (lax.all_gather(v, "fs", axis=0, tiled=True) for v in (gate_weight, up_weight))
    down = lax.all_gather(down_weight, "fs", axis=1, tiled=True)
    gate_pre = jnp.dot(x, gate, preferred_element_type=f32)
    up_pre = jnp.dot(x, up, preferred_element_type=f32)
    grad_hidden = lax.dot_general(c, down, last, preferred_element_type=f32)
    sigmoid_gate = jax.nn.sigmoid(gate_pre)
    activated = gate_pre * sigmoid_gate
    hidden = (activated * up_pre).astype(bf16)
    grad_gate = (
        grad_hidden * up_pre * sigmoid_gate * (1.0 + gate_pre * (1.0 - sigmoid_gate))
    ).astype(bf16)
    grad_up = (grad_hidden * activated).astype(bf16)
    partial_sum = lax.dot_general(grad_gate, gate, last, preferred_element_type=f32)
    partial_sum += lax.dot_general(grad_up, up, last, preferred_element_type=f32)
    grad_inputs = lax.psum_scatter(partial_sum, "tp", scatter_dimension=1, tiled=True)

    def scattered(lhs, rhs, dimension):
        grads = lax.dot_general(lhs, rhs, first, preferred_element_type=f32)
        grads = lax.psum_scatter(grads, "fs", scatter_dimension=dimension, tiled=True)
        return lax.psum(grads, "rep")

    return (
        grad_inputs.astype(bf16),
        scattered(x, grad_gate, 0),
        scattered(x, grad_up, 0),
        scattered(hidden, c, 1),
    )


def per_device(n_rep, n_fs, n_tp, x, c, gate_weight, up_weight, down_weight):
    n_y = max(k for k in range(1, n_fs + 1) if n_fs % k == 0 and k * k <= n_fs)
    n_z = n_fs // n_y
    tokens, width = x.shape
    depth, hidden_tp = gate_weight.shape
    args = (x, c, gate_weight, up_weight, down_weight)
    whole = hidden_tp % (16 * n_rep * n_z) == 0
    if whole and tokens % 128 == width % 128 == depth % 128 == 0 and min(n_rep, n_y, n_tp) > 1:
        return fused((n_rep, n_fs, n_tp, n_y), *args)
    return gathered(*args)


def solution(mesh):
    n_rep, n_fs, n_tp = (mesh.shape[axis] for axis in ("rep", "fs", "tp"))
    placed = (
        P(("rep", "fs"), "tp"),
        P(("rep", "fs"), "tp"),
        P("fs", "tp"),
        P("fs", "tp"),
        P("tp", "fs"),
    )
    return jax.shard_map(
        functools.partial(per_device, n_rep, n_fs, n_tp),
        mesh=mesh,
        in_specs=placed,
        out_specs=(P(("rep", "fs"), "tp"), P("fs", "tp"), P("fs", "tp"), P("tp", "fs")),
        check_vma=False,
    )
```

```python
import functools

import jax
import jax.numpy as jnp
from jax import lax
from jax.experimental import pallas as pl
from jax.experimental.pallas import tpu as pltpu
from jax.sharding import PartitionSpec as P

MESH = pl.DeviceIdType.MESH


def greet(n_rep, n_fs, n_tp):
    barrier = pltpu.get_barrier_semaphore()
    for axis, n in (("rep", n_rep), ("fs", n_fs), ("tp", n_tp)):
        me = lax.axis_index(axis)
        for k in range(1, n):
            pl.semaphore_signal(
                barrier, inc=1, device_id={axis: lax.rem(me + k, n)}, device_id_type=MESH
            )
    return lambda: pl.semaphore_wait(barrier, n_rep + n_fs + n_tp - 3)


class Sender:
    def __init__(self, sems):
        self.sems, self.used, self.pending = sems, 0, []

    def run(self, build, when):
        if when is None:
            build().start()
        else:
            pl.when(when)(lambda: build().start())

    def send(self, src, dst, recv_sem, axis, peer, when=None):
        def build(at=self.used):
            return pltpu.make_async_remote_copy(
                src_ref=src,
                dst_ref=dst,
                send_sem=self.sems.at[at],
                recv_sem=recv_sem,
                device_id={axis: peer},
                device_id_type=MESH,
            )

        self.used += 1
        self.run(build, when)
        self.pending.append((lambda: build().wait_send(), when))

    def local(self, src, dst):
        def build(at=self.used):
            return pltpu.make_async_copy(src, dst, self.sems.at[at])

        self.used += 1
        self.run(build, None)
        self.pending.append((lambda: build().wait(), None))

    def finish(self):
        for wait, when in self.pending:
            if when is None:
                wait()
            else:
                pl.when(when)(wait)
        self.used, self.pending = 0, []


def arrived(slot, recv_sem, when=None):
    def wait():
        pltpu.make_async_copy(slot, slot, recv_sem).wait()

    if when is None:
        wait()
    else:
        pl.when(when)(wait)


def near_first(n):
    return sorted(range(1, n), key=lambda k: min(k, n - k))


def layer_kernel(
    sizes, *refs
):
    inputs, rest = refs[:5], refs[5:]
    outputs, local, loads, rest = rest[:4], rest[4:9], rest[9], rest[10:]
    met = greet(*sizes[:3])
    copies = [pltpu.make_async_copy(a, b, loads.at[i]) for i, (a, b) in enumerate(zip(inputs, local))]
    for copy in copies:
        copy.start()
    met()
    layer(sizes, copies, *local, *outputs, *rest)


def layer(
    sizes, copies, x_ref, c_ref, gate_ref, up_ref, down_ref, dx_ref, dgate_ref, dup_ref, ddown_ref,
    xa, ca, wt, wa, wa_more, pre, pre_down, gt, ht,
    p, p_in, q, x_in, r, z_in, total,
    gp, go, g_in, gs, dw, gp_more, go_more, g_in_more, gs_more, dw_more,
    sends, act_recv, w_recv, p_recv, x_recv, z_recv, g_recv, d_recv,
):
    n_rep, n_fs, n_tp, n_y = sizes
    n_z = n_fs // n_y
    f32, bf16 = jnp.float32, jnp.bfloat16
    rep, fs, tp = (lax.axis_index(axis) for axis in ("rep", "fs", "tp"))
    z, y = fs // n_y, lax.rem(fs, n_y)
    tokens, width = x_ref.shape
    base, more, depth = wa.shape[1], ht.shape[0] - wa.shape[1], down_ref.shape[1]
    units = base + more
    inner = jnp.logical_and(z > 0, z < n_z - 1) if more else None
    out = Sender(sends)

    def span(at, size):
        return pl.ds(pl.multiple_of(at * size, size), size)

    def peers(me, n):
        return [lax.rem(me + k, n) for k in range(1, n)]

    def at_z(other, row=y):
        return other * n_y + row

    far_first, low, high = [], 0, n_z - 1
    for _ in range(n_z):
        above = 2 * (high - z) + jnp.where(2 * z < n_z, 1, 0) > 2 * (z - low)
        far_first.append(jnp.where(above, high, low))
        low, high = jnp.where(above, low, low + 1), jnp.where(above, high - 1, high)
    others = far_first[:-1]
    near = [z] + others[::-1]
    halves = 1 if n_z % 2 else 2
    half = n_z // halves
    start = z // half * half
    home = [start + lax.rem(z - start + i, half) for i in range(half)]
    away = [jnp.where(z < half, n_z - 1 - i, i) for i in range(n_z - half)]

    own_acts, acts = (x_ref, c_ref), (xa, ca)

    def act_slot(a, shard, part):
        return acts[a].at[span(shard, tokens), span(part, width)]

    def act_send(a, shard, src, axis, peer, when=None):
        out.send(src, act_slot(a, shard, tp), act_recv.at[a, shard, tp], axis, peer, when)

    def to_rep(a, shard, src, when=None):
        for peer in peers(rep, n_rep):
            act_send(a, shard, src, "rep", peer, when)

    def to_tp(a, shard, src, when=None):
        for peer in peers(tp, n_tp):
            act_send(a, shard, src, "tp", peer, when)

    def from_rep(other):
        for peer in peers(rep, n_rep):
            for a in range(2):
                shard = peer * n_z + other
                slot = act_slot(a, shard, tp)
                arrived(slot, act_recv.at[a, shard, tp])
                to_tp(a, shard, slot)

    mine = rep * n_z + z
    for a in range(2):
        copies[a].wait()
        act_send(a, mine, own_acts[a], "fs", fs + n_y, z + 1 < n_z)
        act_send(a, mine, own_acts[a], "fs", fs - n_y, z >= 1)
        to_rep(a, mine, own_acts[a])
    for a in range(2):
        to_tp(a, mine, own_acts[a])

    for copy in copies[2:]:
        copy.wait()
    wt[0] = gate_ref[...].T
    wt[1] = up_ref[...].T

    def inside(other):
        return jnp.logical_and(other > 0, other < n_z - 1)

    parts = [(0, 0), (0, 1), (1, 0), (1, 1)][: 4 if more else 2]
    here_too = {0: None, 1: inner}

    def w_part(extra, kind, other):
        start = rep * (n_z * base + max(n_z - 2, 0) * more) + other * units
        start = start - (jnp.minimum(other, 1) * more if more else 0) + extra * base
        rows = pl.ds(pl.multiple_of(start, 16), more if extra else base)
        return down_ref.at[rows] if kind else wt.at[:, rows]

    def w_slot(extra, kind, block):
        held = wa_more if extra else wa
        return held.at[2 if kind else slice(0, 2), :, span(block, depth)]

    def w_send(part, block, src, peer, when=None):
        out.send(src, w_slot(*part, block), w_recv.at[parts.index(part), block], "fs", peer, when)

    def w_arrived(part, block):
        arrived(w_slot(*part, block), w_recv.at[parts.index(part), block], here_too[part[0]])

    for part in parts:
        for row in peers(y, n_y):
            w_send(part, fs, w_part(*part, z), at_z(z, row), here_too[part[0]])

    def keep(part):
        held, (extra, kind) = (wa_more if part[0] else wa), part
        if kind:
            held[2, :, span(fs, depth)] = w_part(*part, z)[...]
        else:
            held[0:2, :, span(fs, depth)] = w_part(*part, z)[...]

    for part in parts:
        if part[0]:
            pl.when(inner)(functools.partial(keep, part))
        else:
            keep(part)
    for a in range(2):
        acts[a][span(mine, tokens), span(tp, width)] = own_acts[a][...]

    def send_weights(step, only=None):
        for sign, here in ((1, z + step < n_z), (-1, z >= step)):
            other = z + sign * step
            here = here if only is None else jnp.logical_and(here, only)
            for part in parts:
                when = jnp.logical_and(here, inside(other)) if part[0] else here
                w_send(part, fs, w_part(*part, other), at_z(other), when)

    def swap_weights(other):
        for part in parts:
            block = at_z(other)
            w_arrived(part, block)
            for row in peers(y, n_y):
                w_send(part, block, w_slot(*part, block), at_z(z, row), here_too[part[0]])

    held = n_z > 3
    for k in range(1, n_z):
        for a in range(2):
            for here, onward, step in ((z >= k, z + 1 < n_z, -1), (z + k < n_z, z >= 1, 1)):
                shard = mine + step * k
                slot = act_slot(a, shard, tp)
                arrived(slot, act_recv.at[a, shard, tp], here)
                if k < n_z - 1:
                    act_send(a, shard, slot, "fs", fs - step * n_y, jnp.logical_and(here, onward))
                to_rep(a, shard, slot, here)
                to_tp(a, shard, slot, here)
            if k == n_z - 1 and a == 0:
                send_weights(k)
                for other in home[1:]:
                    from_rep(other)
        if k < n_z - 2 or not held and k == n_z - 2:
            send_weights(k)
        if k == 1:
            from_rep(z)
        if held and k == n_z - 2:
            send_weights(k, jnp.logical_not(inside(z)))
            swap_weights(near[1])
    if n_z == 1:
        from_rep(z)
    if held:
        near[2], near[3] = near[3], near[2]
        swap_weights(near[2])
        swap_weights(near[3])
        send_weights(n_z - 2, inside(z))
    for k in range(4 if held else 1, n_z):
        swap_weights(near[k])
    def acts_arrived(side, places):
        for part in peers(tp, n_tp):
            for other in places:
                for a in range(2):
                    shard = side * n_z + other
                    arrived(act_slot(a, shard, part), act_recv.at[a, shard, part])

    last = (((1,), (1,)), ((), ()))
    first = (((0,), (0,)), ((), ()))

    def by_place(work):
        if not more:
            work(False)
        else:
            pl.when(inner)(lambda: work(True))
            pl.when(jnp.logical_not(inner))(lambda: work(False))

    def weights(full, kind, cols):
        rows = slice(2, 3) if kind else slice(0, 2)
        value = wa[rows, :, cols]
        value = value.reshape(-1, value.shape[-1])
        if full:
            extra = wa_more[rows, :, cols]
            value = jnp.concatenate([value, extra.reshape(-1, value.shape[-1])], axis=0)
        return value

    def tokens_of(side, away):
        place = z // half
        return span(side * halves + (1 - place if away else place), half * tokens)

    def contract(block, groups, fresh):
        cols = span(block, depth)

        def work(full):
            for kind, ref, act in ((0, pre, xa), (1, pre_down, ca)):
                lhs = weights(full, kind, cols)
                rows = slice(0, lhs.shape[0])
                for group in groups:
                    at = tokens_of(*group)
                    part = lax.dot_general(lhs, act[at, cols], last, preferred_element_type=f32)
                    ref[rows, at] = part if fresh else ref[rows, at] + part

        by_place(work)

    sides = peers(rep, n_rep)
    soon = [(side, False) for side in sides + [rep]]
    late = []
    for side in sides + [rep]:
        acts_arrived(side, home)
    if away:
        acts_arrived(rep, away)
        soon.append((rep, True))
        late = [(side, True) for side in sides]
    blocks = []
    for k in range(n_z):
        if k == n_z // 2:
            for other in away:
                from_rep(other)
        blocks.append(at_z(near[k]))
        contract(blocks[-1], soon, k == 0)
        for row in peers(y, n_y):
            blocks.append(at_z(near[k], row))
            for part in parts:
                w_arrived(part, blocks[-1])
            contract(blocks[-1], soon, False)
    out.finish()

    def activate(group):
        cols = tokens_of(*group)

        def rows_of(start, size, down):
            @pl.loop(0, size // 16)
            def _(step):
                gate = pl.ds(pl.multiple_of(start + step * 16, 16), 16)
                up = pl.ds(pl.multiple_of(start + size + step * 16, 16), 16)
                rows = pl.ds(pl.multiple_of(down + step * 16, 16), 16)
                gate_pre, up_pre, grad_hidden = pre[gate, cols], pre[up, cols], pre_down[rows, cols]
                sigmoid_gate = jax.nn.sigmoid(gate_pre)
                activated = gate_pre * sigmoid_gate
                ht[rows, cols] = (activated * up_pre).astype(bf16)
                gt[gate, cols] = (
                    grad_hidden * up_pre * sigmoid_gate * (1.0 + gate_pre * (1.0 - sigmoid_gate))
                ).astype(bf16)
                gt[up, cols] = (grad_hidden * activated).astype(bf16)

        rows_of(0, base, 0)
        if more:
            pl.when(inner)(lambda: rows_of(2 * base, more, base))

    def partial_inputs(group):
        rows = tokens_of(*group)

        def work(full):
            rhs = weights(full, 0, slice(None))
            p[rows] = lax.dot_general(
                gt[: rhs.shape[0], rows], rhs, first, preferred_element_type=f32
            ).astype(bf16)

        by_place(work)
        for other in away if group[1] else home[1:] + home[:1]:
            shard = group[0] * n_z + other
            for j in range(1, n_tp):
                peer = lax.rem(tp + j, n_tp)
                out.send(
                    p.at[span(shard, tokens), span(peer, width)],
                    p_in.at[j - 1, shard],
                    p_recv.at[j - 1, shard],
                    "tp",
                    peer,
                )

    def pair_wait(shard):
        for j in range(n_tp - 1):
            arrived(p_in.at[j, shard], p_recv.at[j, shard])

    def pair_sum(shard):
        value = p[span(shard, tokens), span(tp, width)].astype(f32)
        for j in range(n_tp - 1):
            value = value + p_in[j, shard].astype(f32)
        return value

    def weight_block(block, dst, dst_more):
        cols = span(block, depth)

        def work(full):
            held = units if full else base
            both = jnp.dot(gt[: 2 * held], xa[:, cols], preferred_element_type=f32)
            down = jnp.dot(ht[:held], ca[:, cols], preferred_element_type=f32)
            dst[: 2 * base] = both[: 2 * base].astype(dst.dtype)
            dst[2 * base :] = down[:base].astype(dst.dtype)
            if full:
                dst_more[: 2 * more] = both[2 * base :].astype(dst.dtype)
                dst_more[2 * more :] = down[base:].astype(dst.dtype)

        by_place(work)

    def rep_sum(other):
        value = pair_sum(rep * n_z + other)
        for j in range(n_rep - 1):
            value = value + x_in[j, other].astype(f32)
        return value

    def rep_wait(other):
        for j in range(n_rep - 1):
            arrived(x_in.at[j, other], x_recv.at[j, other])

    def toward(other, passing):
        up = other > z
        came = jnp.where(up, 0, 1)
        behind = jnp.where(up, z >= 1, z + 1 < n_z)
        when = behind if passing else jnp.logical_not(behind)
        slot, recv_sem = z_in.at[came, other], z_recv.at[came, other]

        @pl.when(when)
        def _():
            rep_wait(other)
            value = rep_sum(other)
            if passing:
                arrived(slot, recv_sem)
                value = value + slot[...].astype(f32)
            r[other] = value.astype(bf16)

        peer = jnp.where(up, fs + n_y, fs - n_y)
        out.send(r.at[other], slot, recv_sem, "fs", peer, when)

    sets = [(gp, go, g_in, gs, dw)]
    if more:
        sets.append((gp_more, go_more, g_in_more, gs_more, dw_more))

    def dw_slot(extra, side, other):
        if extra:
            other = jnp.clip(other - 1, 0, n_z - 3)
            return dw_more.at[side * (n_z - 2) + other]
        return dw.at[side * n_z + other]

    def dw_send(extra, other, when):
        slot = dw_slot(extra, rep, other)
        for peer in peers(rep, n_rep):
            out.send(slot, slot, d_recv.at[extra, rep, other], "rep", peer, when)

    def g_step(other, own):
        def work(extra):
            partial, total, came, summed, _ = sets[extra]
            total = total[other]
            for j in range(n_y - 1):
                arrived(came.at[j, other], g_recv.at[extra, j, other])
                total = total + came[j, other].astype(f32)
            if own:
                dw_slot(extra, rep, z)[...] = total.astype(bf16)
            else:
                summed[other] = total.astype(bf16)

        for extra in range(len(sets)):
            if extra:
                pl.when(inner)(lambda: work(1))
            else:
                work(0)
            if own:
                dw_send(extra, z, here_too[extra])
            else:
                out.send(
                    sets[extra][3].at[other], dw_slot(extra, rep, z), d_recv.at[extra, rep, z],
                    "fs", at_z(other), here_too[extra],
                )

    def g_forward(other):
        for extra in range(len(sets)):
            when = inside(other) if extra else None
            arrived(dw_slot(extra, rep, other), d_recv.at[extra, rep, other], when)
            dw_send(extra, other, when)

    def to_row(other):
        for j in range(1, n_y):
            row = lax.rem(y + j, n_y)
            at = (j - 1, other)
            weight_block(at_z(other, row), gp.at[at], gp_more.at[at])
            for extra, (partial, _, came, *_) in enumerate(sets):
                out.send(
                    partial.at[at], came.at[at], g_recv.at[extra, j - 1, other],
                    "fs", at_z(z, row), here_too[extra],
                )

    def to_side(other):
        for j in range(1, n_rep):
            side = lax.rem(rep + j, n_rep)
            pair_wait(side * n_z + other)
            q[j - 1, other] = pair_sum(side * n_z + other).astype(bf16)
            out.send(
                q.at[j - 1, other], x_in.at[j - 1, other], x_recv.at[j - 1, other], "rep", side
            )

    for group in soon[: len(sides)]:
        activate(group)
        partial_inputs(group)
    for group in soon[len(sides) :]:
        activate(group)
    for side, _ in late:
        acts_arrived(side, away)
    for i, block in enumerate(blocks if late else ()):
        contract(block, late, i == 0)
    for other in home[1:]:
        to_side(other)
    for group in late:
        activate(group)
        partial_inputs(group)
    rows = others[:-1] + [z] + others[-1:]
    to_row(rows[0])
    for other in away + [z]:
        to_side(other)
    for other in rows[1:]:
        to_row(other)
    for group in soon[len(sides) :]:
        partial_inputs(group)
    for other in rows:
        weight_block(at_z(other), go.at[other], go_more.at[other])
    for other in far_first:
        pair_wait(rep * n_z + other)

    for i, other in enumerate(others[:-1]):
        g_step(other, False)
        if i == 0:
            toward(other, False)
    for other in others[:1]:
        toward(other, True)
    g_step(z, True)
    for other in others[1:2]:
        g_forward(other)
        toward(other, False)
    for other in others[-1:]:
        g_step(other, False)
    for other in others[2:]:
        toward(other, False)
    for other in others[:1]:
        g_forward(other)
    for other in others[1:][-1:]:
        toward(other, True)
    for other in others[2:]:
        g_forward(other)
    for other in others[1:-1]:
        toward(other, True)
    rep_wait(z)
    total[...] = rep_sum(z)
    for came, here in ((0, z >= 1), (1, z + 1 < n_z)):

        @pl.when(here)
        def _(came=came):
            arrived(z_in.at[came, z], z_recv.at[came, z])
            total[...] = total[...] + z_in[came, z].astype(f32)

    dx_ref[...] = total[...].astype(bf16)
    for side in peers(rep, n_rep):
        for other in [z] + others:
            for extra in range(len(sets)):
                arrived(
                    dw_slot(extra, side, other), d_recv.at[extra, side, other],
                    inside(other) if extra else None,
                )

    def gathered_rows(kind):
        rows = []
        for side in range(n_rep):
            for other in range(n_z):
                rows.append(dw[side * n_z + other, kind * base : (kind + 1) * base])
                if more and 0 < other < n_z - 1:
                    at = side * (n_z - 2) + other - 1
                    rows.append(dw_more[at, kind * more : (kind + 1) * more])
        return jnp.concatenate(rows, axis=0)

    dgate_ref[...] = gathered_rows(0).T
    dup_ref[...] = gathered_rows(1).T
    ddown_ref[...] = gathered_rows(2)
    out.finish()


VMEM = pl.BlockSpec(memory_space=pltpu.VMEM)
ANY = pl.BlockSpec(memory_space=pl.ANY)
DMA = pltpu.SemaphoreType.DMA


def widen_kernel(*refs):
    for src, dst in zip(refs[:4], refs[4:]):
        dst[...] = src[...].astype(dst.dtype)


def fused(sizes, x, c, gate_weight, up_weight, down_weight):
    bf16, f32 = jnp.bfloat16, jnp.float32
    n_rep, n_fs, n_tp, n_y = sizes
    n_z = n_fs // n_y
    tokens, width = x.shape
    depth, hidden_tp = gate_weight.shape
    model, per_rep = width * n_tp, hidden_tp // n_rep
    base, more = per_rep // n_z, 0
    for size in range(16, per_rep, 16) if n_z > 2 else ():
        rest = per_rep - (n_z - 2) * size
        if rest % (16 * n_z) == 0 and 4 * size * n_z <= 5 * rest:
            base, more = rest // n_z, size
    units, spare, mids = base + more, max(more, 16), max(n_z - 2, 1)
    kinds = 4 if more else 2
    shards = n_rep * n_z
    group = shards * tokens
    tp_rep = n_tp + n_rep - 2
    n_sends = (
        2 * (2 + tp_rep) + 4 * ((n_z - 1) * (1 + tp_rep) - 1) + 2 * n_z * (n_rep - 1) * (n_tp - 1)
        + kinds * (n_y - 1) * n_z + 2 * kinds * (n_z - 1 + (n_z > 3))
    )
    grad_inputs, *grads = pl.pallas_call(
        functools.partial(layer_kernel, sizes),
        out_shape=(
            jax.ShapeDtypeStruct((tokens, width), bf16),
            jax.ShapeDtypeStruct((depth, hidden_tp), bf16),
            jax.ShapeDtypeStruct((depth, hidden_tp), bf16),
            jax.ShapeDtypeStruct((hidden_tp, depth), bf16),
        ),
        in_specs=[ANY] * 5,
        out_specs=(VMEM,) * 4,
        scratch_shapes=[
            *(pltpu.VMEM(v.shape, bf16) for v in (x, c, gate_weight, up_weight, down_weight)),
            DMA((5,)),
            pltpu.VMEM((group, model), bf16),
            pltpu.VMEM((group, model), bf16),
            pltpu.VMEM((2, hidden_tp, depth), bf16),
            pltpu.VMEM((3, base, model), bf16),
            pltpu.VMEM((3, spare, model), bf16),
            pltpu.VMEM((2 * units, group), f32),
            pltpu.VMEM((units, group), f32),
            pltpu.VMEM((2 * units, group), bf16),
            pltpu.VMEM((units, group), bf16),
            pltpu.VMEM((group, model), bf16),
            pltpu.VMEM((n_tp - 1, shards, tokens, width), bf16),
            pltpu.VMEM((n_rep - 1, n_z, tokens, width), bf16),
            pltpu.VMEM((n_rep - 1, n_z, tokens, width), bf16),
            pltpu.VMEM((n_z, tokens, width), bf16),
            pltpu.VMEM((2, n_z, tokens, width), bf16),
            pltpu.VMEM((tokens, width), f32),
            *(
                pltpu.VMEM((*lead, 3 * size, depth), kind)
                for size, places in ((base, shards), (spare, n_rep * mids))
                for lead, kind in (
                    ((n_y - 1, n_z), bf16), ((n_z,), f32), ((n_y - 1, n_z), bf16),
                    ((n_z,), bf16), ((places,), bf16),
                )
            ),
            DMA((n_sends,)),
            DMA((2, shards, n_tp)),
            DMA((kinds, n_fs)),
            DMA((n_tp - 1, shards)),
            DMA((n_rep - 1, n_z)),
            DMA((2, n_z)),
            DMA((kinds // 2, n_y - 1, n_z)),
            DMA((kinds // 2, n_rep, n_z)),
        ],
        compiler_params=pltpu.CompilerParams(
            collective_id=0, has_side_effects=True, vmem_limit_bytes=60 * 2**20
        ),
    )(x, c, gate_weight, up_weight, down_weight)
    steps = 2

    def block(shape):
        return pl.BlockSpec((shape[0] // steps, shape[1]), lambda i: (i, 0))

    results = (grad_inputs, *grads)
    return pl.pallas_call(
        widen_kernel,
        grid=(steps,),
        out_shape=[
            jax.ShapeDtypeStruct(v.shape, f32 if i else bf16) for i, v in enumerate(results)
        ],
        in_specs=[block(v.shape) for v in results],
        out_specs=[block(v.shape) for v in results],
    )(*results)


def gathered(x, c, gate_weight, up_weight, down_weight):
    bf16, f32 = jnp.bfloat16, jnp.float32
    last = (((1,), (1,)), ((), ()))
    first = (((0,), (0,)), ((), ()))
    x, c = (lax.all_gather(v, "tp", axis=1, tiled=True) for v in (x, c))
    gate, up = (lax.all_gather(v, "fs", axis=0, tiled=True) for v in (gate_weight, up_weight))
    down = lax.all_gather(down_weight, "fs", axis=1, tiled=True)
    gate_pre = jnp.dot(x, gate, preferred_element_type=f32)
    up_pre = jnp.dot(x, up, preferred_element_type=f32)
    grad_hidden = lax.dot_general(c, down, last, preferred_element_type=f32)
    sigmoid_gate = jax.nn.sigmoid(gate_pre)
    activated = gate_pre * sigmoid_gate
    hidden = (activated * up_pre).astype(bf16)
    grad_gate = (
        grad_hidden * up_pre * sigmoid_gate * (1.0 + gate_pre * (1.0 - sigmoid_gate))
    ).astype(bf16)
    grad_up = (grad_hidden * activated).astype(bf16)
    partial_sum = lax.dot_general(grad_gate, gate, last, preferred_element_type=f32)
    partial_sum += lax.dot_general(grad_up, up, last, preferred_element_type=f32)
    grad_inputs = lax.psum_scatter(partial_sum, "tp", scatter_dimension=1, tiled=True)

    def scattered(lhs, rhs, dimension):
        grads = lax.dot_general(lhs, rhs, first, preferred_element_type=f32)
        grads = lax.psum_scatter(grads, "fs", scatter_dimension=dimension, tiled=True)
        return lax.psum(grads, "rep")

    return (
        grad_inputs.astype(bf16),
        scattered(x, grad_gate, 0),
        scattered(x, grad_up, 0),
        scattered(hidden, c, 1),
    )


def per_device(n_rep, n_fs, n_tp, x, c, gate_weight, up_weight, down_weight):
    n_y = max(k for k in range(1, n_fs + 1) if n_fs % k == 0 and k * k <= n_fs)
    n_z = n_fs // n_y
    tokens, width = x.shape
    depth, hidden_tp = gate_weight.shape
    args = (x, c, gate_weight, up_weight, down_weight)
    whole = hidden_tp % (16 * n_rep * n_z) == 0
    if whole and tokens % 128 == width % 128 == depth % 128 == 0 and min(n_rep, n_y, n_tp) > 1:
        return fused((n_rep, n_fs, n_tp, n_y), *args)
    return gathered(*args)


def solution(mesh):
    n_rep, n_fs, n_tp = (mesh.shape[axis] for axis in ("rep", "fs", "tp"))
    placed = (
        P(("rep", "fs"), "tp"),
        P(("rep", "fs"), "tp"),
        P("fs", "tp"),
        P("fs", "tp"),
        P("tp", "fs"),
    )
    return jax.shard_map(
        functools.partial(per_device, n_rep, n_fs, n_tp),
        mesh=mesh,
        in_specs=placed,
        out_specs=(P(("rep", "fs"), "tp"), P("fs", "tp"), P("fs", "tp"), P("tp", "fs")),
        check_vma=False,
    )
```

```python
import functools

import jax
import jax.numpy as jnp
from jax import lax
from jax.experimental import pallas as pl
from jax.experimental.pallas import tpu as pltpu
from jax.sharding import PartitionSpec as P

MESH = pl.DeviceIdType.MESH


def greet(n_rep, n_fs, n_tp):
    barrier = pltpu.get_barrier_semaphore()
    for axis, n in (("rep", n_rep), ("fs", n_fs), ("tp", n_tp)):
        me = lax.axis_index(axis)
        for k in range(1, n):
            pl.semaphore_signal(
                barrier, inc=1, device_id={axis: lax.rem(me + k, n)}, device_id_type=MESH
            )
    return lambda: pl.semaphore_wait(barrier, n_rep + n_fs + n_tp - 3)


class Sender:
    def __init__(self, sems):
        self.sems, self.used, self.pending = sems, 0, []

    def run(self, build, when):
        if when is None:
            build().start()
        else:
            pl.when(when)(lambda: build().start())

    def send(self, src, dst, recv_sem, axis, peer, when=None):
        def build(at=self.used):
            return pltpu.make_async_remote_copy(
                src_ref=src,
                dst_ref=dst,
                send_sem=self.sems.at[at],
                recv_sem=recv_sem,
                device_id={axis: peer},
                device_id_type=MESH,
            )

        self.used += 1
        self.run(build, when)
        self.pending.append((lambda: build().wait_send(), when))

    def local(self, src, dst):
        def build(at=self.used):
            return pltpu.make_async_copy(src, dst, self.sems.at[at])

        self.used += 1
        self.run(build, None)
        self.pending.append((lambda: build().wait(), None))

    def finish(self):
        for wait, when in self.pending:
            if when is None:
                wait()
            else:
                pl.when(when)(wait)
        self.used, self.pending = 0, []


def arrived(slot, recv_sem, when=None):
    def wait():
        pltpu.make_async_copy(slot, slot, recv_sem).wait()

    if when is None:
        wait()
    else:
        pl.when(when)(wait)


def near_first(n):
    return sorted(range(1, n), key=lambda k: min(k, n - k))


def layer_kernel(
    sizes, *refs
):
    inputs, rest = refs[:5], refs[5:]
    outputs, local, loads, rest = rest[:4], rest[4:9], rest[9], rest[10:]
    met = greet(*sizes[:3])
    copies = [pltpu.make_async_copy(a, b, loads.at[i]) for i, (a, b) in enumerate(zip(inputs, local))]
    for copy in copies:
        copy.start()
    met()
    layer(sizes, copies, *local, *outputs, *rest)


def layer(
    sizes, copies, x_ref, c_ref, gate_ref, up_ref, down_ref, dx_ref, dgate_ref, dup_ref, ddown_ref,
    xa, ca, wt, wa, wa_more, pre, pre_down, gt, ht,
    p, p_in, q, x_in, r, z_in, total, h, h_in,
    gp, go, g_in, gs, dw, gp_more, go_more, g_in_more, gs_more, dw_more,
    sends, act_recv, w_recv, p_recv, x_recv, z_recv, g_recv, d_recv, h_recv,
):
    n_rep, n_fs, n_tp, n_y = sizes
    n_z = n_fs // n_y
    f32, bf16 = jnp.float32, jnp.bfloat16
    rep, fs, tp = (lax.axis_index(axis) for axis in ("rep", "fs", "tp"))
    z, y = fs // n_y, lax.rem(fs, n_y)
    tokens, width = x_ref.shape
    base, more, depth = wa.shape[1], ht.shape[0] - wa.shape[1], down_ref.shape[1]
    units = base + more
    inner = jnp.logical_and(z > 0, z < n_z - 1) if more else None
    out = Sender(sends)

    def span(at, size):
        return pl.ds(pl.multiple_of(at * size, size), size)

    def peers(me, n):
        return [lax.rem(me + k, n) for k in range(1, n)]

    def at_z(other, row=y):
        return other * n_y + row

    far_first, low, high = [], 0, n_z - 1
    for _ in range(n_z):
        above = 2 * (high - z) + jnp.where(2 * z < n_z, 1, 0) > 2 * (z - low)
        far_first.append(jnp.where(above, high, low))
        low, high = jnp.where(above, low, low + 1), jnp.where(above, high - 1, high)
    others = far_first[:-1]
    near = [z] + others[::-1]
    halves = 1 if n_z % 2 else 2
    half = n_z // halves
    start = z // half * half
    home = [start + lax.rem(z - start + i, half) for i in range(half)]
    away = [jnp.where(z < half, n_z - 1 - i, i) for i in range(n_z - half)]

    own_acts, acts = (x_ref, c_ref), (xa, ca)

    def act_slot(a, shard, part):
        return acts[a].at[span(shard, tokens), span(part, width)]

    def act_send(a, shard, src, axis, peer, when=None):
        out.send(src, act_slot(a, shard, tp), act_recv.at[a, shard, tp], axis, peer, when)

    def to_rep(a, shard, src, when=None):
        for peer in peers(rep, n_rep):
            act_send(a, shard, src, "rep", peer, when)

    def to_tp(a, shard, src, when=None):
        for peer in peers(tp, n_tp):
            act_send(a, shard, src, "tp", peer, when)

    def from_rep(other, only=None):
        for peer in peers(rep, n_rep):
            for a in range(2):
                shard = peer * n_z + other
                slot = act_slot(a, shard, tp)
                arrived(slot, act_recv.at[a, shard, tp], only)
                to_tp(a, shard, slot, only)

    mine = rep * n_z + z
    for a in range(2):
        copies[a].wait()
        act_send(a, mine, own_acts[a], "fs", fs + n_y, z + 1 < n_z)
        act_send(a, mine, own_acts[a], "fs", fs - n_y, z >= 1)
        to_rep(a, mine, own_acts[a])
    for a in range(2):
        to_tp(a, mine, own_acts[a])

    for copy in copies[2:]:
        copy.wait()
    wt[0] = gate_ref[...].T
    wt[1] = up_ref[...].T

    def inside(other):
        return jnp.logical_and(other > 0, other < n_z - 1)

    parts = [(0, 0), (0, 1), (1, 0), (1, 1)][: 4 if more else 2]
    here_too = {0: None, 1: inner}

    def w_part(extra, kind, other):
        start = rep * (n_z * base + max(n_z - 2, 0) * more) + other * units
        start = start - (jnp.minimum(other, 1) * more if more else 0) + extra * base
        rows = pl.ds(pl.multiple_of(start, 16), more if extra else base)
        return down_ref.at[rows] if kind else wt.at[:, rows]

    def w_slot(extra, kind, block):
        held = wa_more if extra else wa
        return held.at[2 if kind else slice(0, 2), :, span(block, depth)]

    def w_send(part, block, src, peer, when=None):
        out.send(src, w_slot(*part, block), w_recv.at[parts.index(part), block], "fs", peer, when)

    def w_arrived(part, block):
        arrived(w_slot(*part, block), w_recv.at[parts.index(part), block], here_too[part[0]])

    for part in parts:
        for row in peers(y, n_y):
            w_send(part, fs, w_part(*part, z), at_z(z, row), here_too[part[0]])

    def keep(part):
        held, (extra, kind) = (wa_more if part[0] else wa), part
        if kind:
            held[2, :, span(fs, depth)] = w_part(*part, z)[...]
        else:
            held[0:2, :, span(fs, depth)] = w_part(*part, z)[...]

    for part in parts:
        if part[0]:
            pl.when(inner)(functools.partial(keep, part))
        else:
            keep(part)
    for a in range(2):
        acts[a][span(mine, tokens), span(tp, width)] = own_acts[a][...]

    def send_weights(step, only=None):
        for sign, here in ((1, z + step < n_z), (-1, z >= step)):
            other = z + sign * step
            here = here if only is None else jnp.logical_and(here, only)
            for part in parts:
                when = jnp.logical_and(here, inside(other)) if part[0] else here
                w_send(part, fs, w_part(*part, other), at_z(other), when)

    def swap_weights(other):
        for part in parts:
            block = at_z(other)
            w_arrived(part, block)
            for row in peers(y, n_y):
                w_send(part, block, w_slot(*part, block), at_z(z, row), here_too[part[0]])

    held = n_z > 3
    for k in range(1, n_z):
        for a in range(2):
            for here, onward, step in ((z >= k, z + 1 < n_z, -1), (z + k < n_z, z >= 1, 1)):
                shard = mine + step * k
                slot = act_slot(a, shard, tp)
                arrived(slot, act_recv.at[a, shard, tp], here)
                if k < n_z - 1:
                    act_send(a, shard, slot, "fs", fs - step * n_y, jnp.logical_and(here, onward))
                to_rep(a, shard, slot, here)
                to_tp(a, shard, slot, here)
            if k == n_z - 1 and a == 0:
                send_weights(k)
                for other in home[1:]:
                    from_rep(other, jnp.logical_not(inside(z)) if held else None)
        if k < n_z - 2 or not held and k == n_z - 2:
            send_weights(k)
        if k == 1:
            from_rep(z)
        if held and k == n_z - 2:
            send_weights(k, jnp.logical_not(inside(z)))
            swap_weights(near[1])
    if n_z == 1:
        from_rep(z)
    if held:
        near[2], near[3] = near[3], near[2]
        swap_weights(near[2])
        for other in home[1:]:
            from_rep(other, inside(z))
        swap_weights(near[3])
        send_weights(n_z - 2, inside(z))
    for k in range(4 if held else 1, n_z):
        swap_weights(near[k])
    def acts_arrived(side, places):
        for part in peers(tp, n_tp):
            for other in places:
                for a in range(2):
                    shard = side * n_z + other
                    arrived(act_slot(a, shard, part), act_recv.at[a, shard, part])

    last = (((1,), (1,)), ((), ()))
    first = (((0,), (0,)), ((), ()))

    def by_place(work):
        if not more:
            work(False)
        else:
            pl.when(inner)(lambda: work(True))
            pl.when(jnp.logical_not(inner))(lambda: work(False))

    def weights(full, kind, cols):
        rows = slice(2, 3) if kind else slice(0, 2)
        value = wa[rows, :, cols]
        value = value.reshape(-1, value.shape[-1])
        if full:
            extra = wa_more[rows, :, cols]
            value = jnp.concatenate([value, extra.reshape(-1, value.shape[-1])], axis=0)
        return value

    def tokens_of(side, away):
        place = z // half
        return span(side * halves + (1 - place if away else place), half * tokens)

    def contract(block, groups, fresh):
        cols = span(block, depth)

        def work(full):
            for kind, ref, act in ((0, pre, xa), (1, pre_down, ca)):
                lhs = weights(full, kind, cols)
                rows = slice(0, lhs.shape[0])
                for group in groups:
                    at = tokens_of(*group)
                    part = lax.dot_general(lhs, act[at, cols], last, preferred_element_type=f32)
                    ref[rows, at] = part if fresh else ref[rows, at] + part

        by_place(work)

    sides = peers(rep, n_rep)
    soon = [(side, False) for side in sides + [rep]]
    late = []
    for side in sides + [rep]:
        acts_arrived(side, home)
    if away:
        acts_arrived(rep, away)
        soon.append((rep, True))
        late = [(side, True) for side in sides]
    blocks = []
    for k in range(n_z):
        if k == n_z // 2:
            for other in away:
                from_rep(other)
        blocks.append(at_z(near[k]))
        contract(blocks[-1], soon, k == 0)
        for row in peers(y, n_y):
            blocks.append(at_z(near[k], row))
            for part in parts:
                w_arrived(part, blocks[-1])
            contract(blocks[-1], soon, False)
    out.finish()

    def activate(group):
        cols = tokens_of(*group)

        def rows_of(start, size, down):
            @pl.loop(0, size // 16)
            def _(step):
                gate = pl.ds(pl.multiple_of(start + step * 16, 16), 16)
                up = pl.ds(pl.multiple_of(start + size + step * 16, 16), 16)
                rows = pl.ds(pl.multiple_of(down + step * 16, 16), 16)
                gate_pre, up_pre, grad_hidden = pre[gate, cols], pre[up, cols], pre_down[rows, cols]
                sigmoid_gate = jax.nn.sigmoid(gate_pre)
                activated = gate_pre * sigmoid_gate
                ht[rows, cols] = (activated * up_pre).astype(bf16)
                gt[gate, cols] = (
                    grad_hidden * up_pre * sigmoid_gate * (1.0 + gate_pre * (1.0 - sigmoid_gate))
                ).astype(bf16)
                gt[up, cols] = (grad_hidden * activated).astype(bf16)

        rows_of(0, base, 0)
        if more:
            pl.when(inner)(lambda: rows_of(2 * base, more, base))

    def partial_inputs(group):
        rows = tokens_of(*group)

        def work(full):
            rhs = weights(full, 0, slice(None))
            p[rows] = lax.dot_general(
                gt[: rhs.shape[0], rows], rhs, first, preferred_element_type=f32
            ).astype(bf16)

        by_place(work)
        for other in away if group[1] else home[1:] + home[:1]:
            shard = group[0] * n_z + other
            for j in range(1, n_tp):
                peer = lax.rem(tp + j, n_tp)
                out.send(
                    p.at[span(shard, tokens), span(peer, width)],
                    p_in.at[j - 1, shard],
                    p_recv.at[j - 1, shard],
                    "tp",
                    peer,
                )

    def pair_wait(shard):
        for j in range(n_tp - 1):
            arrived(p_in.at[j, shard], p_recv.at[j, shard])

    def pair_sum(shard):
        value = p[span(shard, tokens), span(tp, width)].astype(f32)
        for j in range(n_tp - 1):
            value = value + p_in[j, shard].astype(f32)
        return value

    def weight_block(block, dst, dst_more):
        cols = span(block, depth)

        def work(full):
            held = units if full else base
            both = jnp.dot(gt[: 2 * held], xa[:, cols], preferred_element_type=f32)
            down = jnp.dot(ht[:held], ca[:, cols], preferred_element_type=f32)
            dst[: 2 * base] = both[: 2 * base].astype(dst.dtype)
            dst[2 * base :] = down[:base].astype(dst.dtype)
            if full:
                dst_more[: 2 * more] = both[2 * base :].astype(dst.dtype)
                dst_more[2 * more :] = down[base:].astype(dst.dtype)

        by_place(work)

    paired = n_z == 4
    if paired:
        taken = jnp.where(inside(z), away[0], away[1])
        given = jnp.where(inside(z), away[1], away[0])

    def rep_sum(other, from_sides=True):
        value = pair_sum(rep * n_z + other)
        for j in range(n_rep - 1 if from_sides else 0):
            value = value + x_in[j, other].astype(f32)
        return value

    def rep_wait(other):
        for j in range(n_rep - 1):
            arrived(x_in.at[j, other], x_recv.at[j, other])

    def toward(i, passing):
        other = others[i]
        from_sides = not paired or i == 2 or passing == (i == 0)
        up = other > z
        came = jnp.where(up, 0, 1)
        behind = jnp.where(up, z >= 1, z + 1 < n_z)
        when = behind if passing else jnp.logical_not(behind)
        slot, recv_sem = z_in.at[came, other], z_recv.at[came, other]

        @pl.when(when)
        def _():
            if from_sides:
                rep_wait(other)
            value = rep_sum(other, from_sides)
            if passing:
                arrived(slot, recv_sem)
                value = value + slot[...].astype(f32)
            r[other] = value.astype(bf16)

        peer = jnp.where(up, fs + n_y, fs - n_y)
        out.send(r.at[other], slot, recv_sem, "fs", peer, when)

    sets = [(gp, go, g_in, gs, dw)]
    if more:
        sets.append((gp_more, go_more, g_in_more, gs_more, dw_more))

    def dw_slot(extra, side, other):
        if extra:
            other = jnp.clip(other - 1, 0, n_z - 3)
            return dw_more.at[side * (n_z - 2) + other]
        return dw.at[side * n_z + other]

    def dw_send(extra, other, when):
        slot = dw_slot(extra, rep, other)
        for peer in peers(rep, n_rep):
            out.send(slot, slot, d_recv.at[extra, rep, other], "rep", peer, when)

    def g_step(other, own):
        def work(extra):
            partial, total, came, summed, _ = sets[extra]
            total = total[other]
            for j in range(n_y - 1):
                arrived(came.at[j, other], g_recv.at[extra, j, other])
                total = total + came[j, other].astype(f32)
            if own:
                dw_slot(extra, rep, z)[...] = total.astype(bf16)
            else:
                summed[other] = total.astype(bf16)

        for extra in range(len(sets)):
            if extra:
                pl.when(inner)(lambda: work(1))
            else:
                work(0)
            if own:
                dw_send(extra, z, here_too[extra])
            else:
                out.send(
                    sets[extra][3].at[other], dw_slot(extra, rep, z), d_recv.at[extra, rep, z],
                    "fs", at_z(other), here_too[extra],
                )

    def g_forward(other):
        for extra in range(len(sets)):
            when = inside(other) if extra else None
            arrived(dw_slot(extra, rep, other), d_recv.at[extra, rep, other], when)
            dw_send(extra, other, when)

    def to_row(other):
        for j in range(1, n_y):
            row = lax.rem(y + j, n_y)
            at = (j - 1, other)
            weight_block(at_z(other, row), gp.at[at], gp_more.at[at])
            for extra, (partial, _, came, *_) in enumerate(sets):
                out.send(
                    partial.at[at], came.at[at], g_recv.at[extra, j - 1, other],
                    "fs", at_z(z, row), here_too[extra],
                )

    def to_side(other, only=None):
        for j in range(1, n_rep):
            side = lax.rem(rep + j, n_rep)

            def work(j=j, side=side):
                if only is None:
                    pair_wait(side * n_z + other)
                value = pair_sum(side * n_z + other)
                if only is not None:
                    arrived(h_in.at[j - 1], h_recv.at[j - 1])
                    value = value + h_in[j - 1].astype(f32)
                q[j - 1, other] = value.astype(bf16)

            if only is None:
                work()
            else:
                pl.when(only)(work)
            out.send(
                q.at[j - 1, other], x_in.at[j - 1, other], x_recv.at[j - 1, other],
                "rep", side, only,
            )

    def give():
        for j in range(1, n_rep):
            side = lax.rem(rep + j, n_rep)
            for other in away:
                pair_wait(side * n_z + other)
            h[j - 1] = pair_sum(side * n_z + given).astype(bf16)
            out.send(h.at[j - 1], h_in.at[j - 1], h_recv.at[j - 1], "fs", at_z(home[1]))

    for group in soon[: len(sides)]:
        activate(group)
        partial_inputs(group)
    for group in soon[len(sides) :]:
        activate(group)
    for side, _ in late:
        acts_arrived(side, away)
    for i, block in enumerate(blocks if late else ()):
        contract(block, late, i == 0)
    for other in home[1:]:
        to_side(other)
    for group in late:
        activate(group)
        partial_inputs(group)
    rows = others[:-1] + [z] + others[-1:]
    to_row(rows[0])
    if paired:
        to_side(z)
        give()
    for other in [] if paired else away + [z]:
        to_side(other)
    for other in rows[1:]:
        to_row(other)
    for group in soon[len(sides) :]:
        partial_inputs(group)
    for other in rows:
        weight_block(at_z(other), go.at[other], go_more.at[other])
    for other in far_first:
        pair_wait(rep * n_z + other)

    count = len(others)
    if paired:
        toward(0, False)
    for i, other in enumerate(others[:-1]):
        g_step(other, False)
        if paired:
            to_side(taken, inside(z) if i == 0 else jnp.logical_not(inside(z)))
        elif i == 0:
            toward(0, False)
    if count == 1:
        toward(0, False)
    if count:
        toward(0, True)
    g_step(z, True)
    for other in others[-1:]:
        g_step(other, False)
    if count > 1:
        g_forward(others[1])
        toward(1, False)
    for i in range(2, count):
        toward(i, False)
    for other in others[:1]:
        g_forward(other)
    if count > 1:
        toward(count - 1, True)
    for other in others[2:]:
        g_forward(other)
    for i in range(1, count - 1):
        toward(i, True)
    rep_wait(z)
    total[...] = rep_sum(z)
    for came, here in ((0, z >= 1), (1, z + 1 < n_z)):

        @pl.when(here)
        def _(came=came):
            arrived(z_in.at[came, z], z_recv.at[came, z])
            total[...] = total[...] + z_in[came, z].astype(f32)

    dx_ref[...] = total[...].astype(bf16)
    for side in peers(rep, n_rep):
        for other in [z] + others:
            for extra in range(len(sets)):
                arrived(
                    dw_slot(extra, side, other), d_recv.at[extra, side, other],
                    inside(other) if extra else None,
                )

    def gathered_rows(kind):
        rows = []
        for side in range(n_rep):
            for other in range(n_z):
                rows.append(dw[side * n_z + other, kind * base : (kind + 1) * base])
                if more and 0 < other < n_z - 1:
                    at = side * (n_z - 2) + other - 1
                    rows.append(dw_more[at, kind * more : (kind + 1) * more])
        return jnp.concatenate(rows, axis=0)

    dgate_ref[...] = gathered_rows(0).T
    dup_ref[...] = gathered_rows(1).T
    ddown_ref[...] = gathered_rows(2)
    out.finish()


VMEM = pl.BlockSpec(memory_space=pltpu.VMEM)
ANY = pl.BlockSpec(memory_space=pl.ANY)
DMA = pltpu.SemaphoreType.DMA


def widen_kernel(*refs):
    for src, dst in zip(refs[:4], refs[4:]):
        dst[...] = src[...].astype(dst.dtype)


def fused(sizes, x, c, gate_weight, up_weight, down_weight):
    bf16, f32 = jnp.bfloat16, jnp.float32
    n_rep, n_fs, n_tp, n_y = sizes
    n_z = n_fs // n_y
    tokens, width = x.shape
    depth, hidden_tp = gate_weight.shape
    model, per_rep = width * n_tp, hidden_tp // n_rep
    base, more = per_rep // n_z, 0
    for size in range(16, per_rep, 16) if n_z > 2 else ():
        rest = per_rep - (n_z - 2) * size
        if rest % (16 * n_z) == 0 and 4 * size * n_z <= 3 * rest:
            base, more = rest // n_z, size
    units, spare, mids = base + more, max(more, 16), max(n_z - 2, 1)
    kinds = 4 if more else 2
    shards = n_rep * n_z
    group = shards * tokens
    tp_rep = n_tp + n_rep - 2
    n_sends = (
        2 * (2 + tp_rep) + 4 * ((n_z - 1) * (1 + tp_rep) - 1) + 2 * (n_z + n_z // 2) * (n_rep - 1) * (n_tp - 1)
        + kinds * (n_y - 1) * n_z + 2 * kinds * (n_z - 1 + (n_z > 3))
    )
    grad_inputs, *grads = pl.pallas_call(
        functools.partial(layer_kernel, sizes),
        out_shape=(
            jax.ShapeDtypeStruct((tokens, width), bf16),
            jax.ShapeDtypeStruct((depth, hidden_tp), bf16),
            jax.ShapeDtypeStruct((depth, hidden_tp), bf16),
            jax.ShapeDtypeStruct((hidden_tp, depth), bf16),
        ),
        in_specs=[ANY] * 5,
        out_specs=(VMEM,) * 4,
        scratch_shapes=[
            *(pltpu.VMEM(v.shape, bf16) for v in (x, c, gate_weight, up_weight, down_weight)),
            DMA((5,)),
            pltpu.VMEM((group, model), bf16),
            pltpu.VMEM((group, model), bf16),
            pltpu.VMEM((2, hidden_tp, depth), bf16),
            pltpu.VMEM((3, base, model), bf16),
            pltpu.VMEM((3, spare, model), bf16),
            pltpu.VMEM((2 * units, group), f32),
            pltpu.VMEM((units, group), f32),
            pltpu.VMEM((2 * units, group), bf16),
            pltpu.VMEM((units, group), bf16),
            pltpu.VMEM((group, model), bf16),
            pltpu.VMEM((n_tp - 1, shards, tokens, width), bf16),
            pltpu.VMEM((n_rep - 1, n_z, tokens, width), bf16),
            pltpu.VMEM((n_rep - 1, n_z, tokens, width), bf16),
            pltpu.VMEM((n_z, tokens, width), bf16),
            pltpu.VMEM((2, n_z, tokens, width), bf16),
            pltpu.VMEM((tokens, width), f32),
            pltpu.VMEM((n_rep - 1, tokens, width), bf16),
            pltpu.VMEM((n_rep - 1, tokens, width), bf16),
            *(
                pltpu.VMEM((*lead, 3 * size, depth), kind)
                for size, places in ((base, shards), (spare, n_rep * mids))
                for lead, kind in (
                    ((n_y - 1, n_z), bf16), ((n_z,), f32), ((n_y - 1, n_z), bf16),
                    ((n_z,), bf16), ((places,), bf16),
                )
            ),
            DMA((n_sends,)),
            DMA((2, shards, n_tp)),
            DMA((kinds, n_fs)),
            DMA((n_tp - 1, shards)),
            DMA((n_rep - 1, n_z)),
            DMA((2, n_z)),
            DMA((kinds // 2, n_y - 1, n_z)),
            DMA((kinds // 2, n_rep, n_z)),
            DMA((n_rep - 1,)),
        ],
        compiler_params=pltpu.CompilerParams(
            collective_id=0, has_side_effects=True, vmem_limit_bytes=60 * 2**20
        ),
    )(x, c, gate_weight, up_weight, down_weight)
    steps = 2

    def block(shape):
        return pl.BlockSpec((shape[0] // steps, shape[1]), lambda i: (i, 0))

    results = (grad_inputs, *grads)
    return pl.pallas_call(
        widen_kernel,
        grid=(steps,),
        out_shape=[
            jax.ShapeDtypeStruct(v.shape, f32 if i else bf16) for i, v in enumerate(results)
        ],
        in_specs=[block(v.shape) for v in results],
        out_specs=[block(v.shape) for v in results],
    )(*results)


def gathered(x, c, gate_weight, up_weight, down_weight):
    bf16, f32 = jnp.bfloat16, jnp.float32
    last = (((1,), (1,)), ((), ()))
    first = (((0,), (0,)), ((), ()))
    x, c = (lax.all_gather(v, "tp", axis=1, tiled=True) for v in (x, c))
    gate, up = (lax.all_gather(v, "fs", axis=0, tiled=True) for v in (gate_weight, up_weight))
    down = lax.all_gather(down_weight, "fs", axis=1, tiled=True)
    gate_pre = jnp.dot(x, gate, preferred_element_type=f32)
    up_pre = jnp.dot(x, up, preferred_element_type=f32)
    grad_hidden = lax.dot_general(c, down, last, preferred_element_type=f32)
    sigmoid_gate = jax.nn.sigmoid(gate_pre)
    activated = gate_pre * sigmoid_gate
    hidden = (activated * up_pre).astype(bf16)
    grad_gate = (
        grad_hidden * up_pre * sigmoid_gate * (1.0 + gate_pre * (1.0 - sigmoid_gate))
    ).astype(bf16)
    grad_up = (grad_hidden * activated).astype(bf16)
    partial_sum = lax.dot_general(grad_gate, gate, last, preferred_element_type=f32)
    partial_sum += lax.dot_general(grad_up, up, last, preferred_element_type=f32)
    grad_inputs = lax.psum_scatter(partial_sum, "tp", scatter_dimension=1, tiled=True)

    def scattered(lhs, rhs, dimension):
        grads = lax.dot_general(lhs, rhs, first, preferred_element_type=f32)
        grads = lax.psum_scatter(grads, "fs", scatter_dimension=dimension, tiled=True)
        return lax.psum(grads, "rep")

    return (
        grad_inputs.astype(bf16),
        scattered(x, grad_gate, 0),
        scattered(x, grad_up, 0),
        scattered(hidden, c, 1),
    )


def per_device(n_rep, n_fs, n_tp, x, c, gate_weight, up_weight, down_weight):
    n_y = max(k for k in range(1, n_fs + 1) if n_fs % k == 0 and k * k <= n_fs)
    n_z = n_fs // n_y
    tokens, width = x.shape
    depth, hidden_tp = gate_weight.shape
    args = (x, c, gate_weight, up_weight, down_weight)
    whole = hidden_tp % (16 * n_rep * n_z) == 0
    if whole and tokens % 128 == width % 128 == depth % 128 == 0 and min(n_rep, n_y, n_tp) > 1:
        return fused((n_rep, n_fs, n_tp, n_y), *args)
    return gathered(*args)


def solution(mesh):
    n_rep, n_fs, n_tp = (mesh.shape[axis] for axis in ("rep", "fs", "tp"))
    placed = (
        P(("rep", "fs"), "tp"),
        P(("rep", "fs"), "tp"),
        P("fs", "tp"),
        P("fs", "tp"),
        P("tp", "fs"),
    )
    return jax.shard_map(
        functools.partial(per_device, n_rep, n_fs, n_tp),
        mesh=mesh,
        in_specs=placed,
        out_specs=(P(("rep", "fs"), "tp"), P("fs", "tp"), P("fs", "tp"), P("tp", "fs")),
        check_vma=False,
    )
```

```python
import functools

import jax
import jax.numpy as jnp
from jax import lax
from jax.experimental import pallas as pl
from jax.experimental.pallas import tpu as pltpu
from jax.sharding import PartitionSpec as P

MESH = pl.DeviceIdType.MESH


def greet(n_rep, n_fs, n_tp):
    barrier = pltpu.get_barrier_semaphore()
    for axis, n in (("rep", n_rep), ("fs", n_fs), ("tp", n_tp)):
        me = lax.axis_index(axis)
        for k in range(1, n):
            pl.semaphore_signal(
                barrier, inc=1, device_id={axis: lax.rem(me + k, n)}, device_id_type=MESH
            )
    return lambda: pl.semaphore_wait(barrier, n_rep + n_fs + n_tp - 3)


class Sender:
    def __init__(self, sems):
        self.sems, self.used, self.pending = sems, 0, []

    def run(self, build, when):
        if when is None:
            build().start()
        else:
            pl.when(when)(lambda: build().start())

    def send(self, src, dst, recv_sem, axis, peer, when=None):
        def build(at=self.used):
            return pltpu.make_async_remote_copy(
                src_ref=src,
                dst_ref=dst,
                send_sem=self.sems.at[at],
                recv_sem=recv_sem,
                device_id={axis: peer},
                device_id_type=MESH,
            )

        self.used += 1
        self.run(build, when)
        self.pending.append((lambda: build().wait_send(), when))

    def local(self, src, dst):
        def build(at=self.used):
            return pltpu.make_async_copy(src, dst, self.sems.at[at])

        self.used += 1
        self.run(build, None)
        self.pending.append((lambda: build().wait(), None))

    def finish(self):
        for wait, when in self.pending:
            if when is None:
                wait()
            else:
                pl.when(when)(wait)
        self.used, self.pending = 0, []


def arrived(slot, recv_sem, when=None):
    def wait():
        pltpu.make_async_copy(slot, slot, recv_sem).wait()

    if when is None:
        wait()
    else:
        pl.when(when)(wait)


def near_first(n):
    return sorted(range(1, n), key=lambda k: min(k, n - k))


def layer_kernel(
    sizes, *refs
):
    inputs, rest = refs[:5], refs[5:]
    outputs, local, loads, rest = rest[:4], rest[4:9], rest[9], rest[10:]
    met = greet(*sizes[:3])
    copies = [pltpu.make_async_copy(a, b, loads.at[i]) for i, (a, b) in enumerate(zip(inputs, local))]
    for copy in copies:
        copy.start()
    met()
    layer(sizes, copies, *local, *outputs, *rest)


def layer(
    sizes, copies, x_ref, c_ref, gate_ref, up_ref, down_ref, dx_ref, dgate_ref, dup_ref, ddown_ref,
    xa, ca, wt, wa, wa_more, pre, pre_down, gt, ht,
    p, p_in, q, x_in, r, z_in, total, h, h_in,
    gp, go, g_in, gs, dw, gp_more, go_more, g_in_more, gs_more, dw_more,
    sends, act_recv, w_recv, p_recv, x_recv, z_recv, g_recv, d_recv, h_recv,
):
    n_rep, n_fs, n_tp, n_y = sizes
    n_z = n_fs // n_y
    f32, bf16 = jnp.float32, jnp.bfloat16
    rep, fs, tp = (lax.axis_index(axis) for axis in ("rep", "fs", "tp"))
    z, y = fs // n_y, lax.rem(fs, n_y)
    tokens, width = x_ref.shape
    base, more, depth = wa.shape[1], ht.shape[0] - wa.shape[1], down_ref.shape[1]
    units = base + more
    inner = jnp.logical_and(z > 0, z < n_z - 1) if more else None
    out = Sender(sends)

    def span(at, size):
        return pl.ds(pl.multiple_of(at * size, size), size)

    def peers(me, n):
        return [lax.rem(me + k, n) for k in range(1, n)]

    def at_z(other, row=y):
        return other * n_y + row

    far_first, low, high = [], 0, n_z - 1
    for _ in range(n_z):
        above = 2 * (high - z) + jnp.where(2 * z < n_z, 1, 0) > 2 * (z - low)
        far_first.append(jnp.where(above, high, low))
        low, high = jnp.where(above, low, low + 1), jnp.where(above, high - 1, high)
    others = far_first[:-1]
    near = [z] + others[::-1]
    halves = 1 if n_z % 2 else 2
    half = n_z // halves
    start = z // half * half
    home = [start + lax.rem(z - start + i, half) for i in range(half)]
    away = [jnp.where(z < half, n_z - 1 - i, i) for i in range(n_z - half)]

    own_acts, acts = (x_ref, c_ref), (xa, ca)

    def act_slot(a, shard, part):
        return acts[a].at[span(shard, tokens), span(part, width)]

    def act_send(a, shard, src, axis, peer, when=None):
        out.send(src, act_slot(a, shard, tp), act_recv.at[a, shard, tp], axis, peer, when)

    def to_rep(a, shard, src, when=None):
        for peer in peers(rep, n_rep):
            act_send(a, shard, src, "rep", peer, when)

    def to_tp(a, shard, src, when=None):
        for peer in peers(tp, n_tp):
            act_send(a, shard, src, "tp", peer, when)

    def from_rep(other, only=None):
        for peer in peers(rep, n_rep):
            for a in range(2):
                shard = peer * n_z + other
                slot = act_slot(a, shard, tp)
                arrived(slot, act_recv.at[a, shard, tp], only)
                to_tp(a, shard, slot, only)

    mine = rep * n_z + z
    for a in range(2):
        copies[a].wait()
        act_send(a, mine, own_acts[a], "fs", fs + n_y, z + 1 < n_z)
        act_send(a, mine, own_acts[a], "fs", fs - n_y, z >= 1)
        to_rep(a, mine, own_acts[a])
    for a in range(2):
        to_tp(a, mine, own_acts[a])

    for copy in copies[2:]:
        copy.wait()
    wt[0] = gate_ref[...].T
    wt[1] = up_ref[...].T

    def inside(other):
        return jnp.logical_and(other > 0, other < n_z - 1)

    parts = [(0, 0), (0, 1), (1, 0), (1, 1)][: 4 if more else 2]
    here_too = {0: None, 1: inner}

    def w_part(extra, kind, other):
        start = rep * (n_z * base + max(n_z - 2, 0) * more) + other * units
        start = start - (jnp.minimum(other, 1) * more if more else 0) + extra * base
        rows = pl.ds(pl.multiple_of(start, 16), more if extra else base)
        return down_ref.at[rows] if kind else wt.at[:, rows]

    def w_slot(extra, kind, block):
        held = wa_more if extra else wa
        return held.at[2 if kind else slice(0, 2), :, span(block, depth)]

    def w_send(part, block, src, peer, when=None):
        out.send(src, w_slot(*part, block), w_recv.at[parts.index(part), block], "fs", peer, when)

    def w_arrived(part, block):
        arrived(w_slot(*part, block), w_recv.at[parts.index(part), block], here_too[part[0]])

    for part in parts:
        for row in peers(y, n_y):
            w_send(part, fs, w_part(*part, z), at_z(z, row), here_too[part[0]])

    def keep(part):
        held, (extra, kind) = (wa_more if part[0] else wa), part
        if kind:
            held[2, :, span(fs, depth)] = w_part(*part, z)[...]
        else:
            held[0:2, :, span(fs, depth)] = w_part(*part, z)[...]

    for part in parts:
        if part[0]:
            pl.when(inner)(functools.partial(keep, part))
        else:
            keep(part)
    for a in range(2):
        acts[a][span(mine, tokens), span(tp, width)] = own_acts[a][...]

    def send_weights(step, only=None):
        for sign, here in ((1, z + step < n_z), (-1, z >= step)):
            other = z + sign * step
            here = here if only is None else jnp.logical_and(here, only)
            for part in parts:
                when = jnp.logical_and(here, inside(other)) if part[0] else here
                w_send(part, fs, w_part(*part, other), at_z(other), when)

    def swap_weights(other):
        for part in parts:
            block = at_z(other)
            w_arrived(part, block)
            for row in peers(y, n_y):
                w_send(part, block, w_slot(*part, block), at_z(z, row), here_too[part[0]])

    held = n_z > 3
    for k in range(1, n_z):
        for a in range(2):
            for here, onward, step in ((z >= k, z + 1 < n_z, -1), (z + k < n_z, z >= 1, 1)):
                shard = mine + step * k
                slot = act_slot(a, shard, tp)
                arrived(slot, act_recv.at[a, shard, tp], here)
                if k < n_z - 1:
                    act_send(a, shard, slot, "fs", fs - step * n_y, jnp.logical_and(here, onward))
                to_rep(a, shard, slot, here)
                to_tp(a, shard, slot, here)
            if k == n_z - 1 and a == 0:
                send_weights(k)
                for other in home[1:]:
                    from_rep(other, jnp.logical_not(inside(z)) if held else None)
        if k < n_z - 2 or not held and k == n_z - 2:
            send_weights(k)
        if k == 1:
            from_rep(z)
        if held and k == n_z - 2:
            send_weights(k, jnp.logical_not(inside(z)))
            swap_weights(near[1])
    if n_z == 1:
        from_rep(z)
    if held:
        near[2], near[3] = near[3], near[2]
        swap_weights(near[2])
        for other in home[1:]:
            from_rep(other, inside(z))
        swap_weights(near[3])
        send_weights(n_z - 2, inside(z))
    for k in range(4 if held else 1, n_z):
        swap_weights(near[k])
    def acts_arrived(side, places):
        for part in peers(tp, n_tp):
            for other in places:
                for a in range(2):
                    shard = side * n_z + other
                    arrived(act_slot(a, shard, part), act_recv.at[a, shard, part])

    last = (((1,), (1,)), ((), ()))
    first = (((0,), (0,)), ((), ()))

    def by_place(work):
        if not more:
            work(False)
        else:
            pl.when(inner)(lambda: work(True))
            pl.when(jnp.logical_not(inner))(lambda: work(False))

    def weights(full, kind, cols):
        rows = slice(2, 3) if kind else slice(0, 2)
        value = wa[rows, :, cols]
        value = value.reshape(-1, value.shape[-1])
        if full:
            extra = wa_more[rows, :, cols]
            value = jnp.concatenate([value, extra.reshape(-1, value.shape[-1])], axis=0)
        return value

    def tokens_of(side, away):
        place = z // half
        return span(side * halves + (1 - place if away else place), half * tokens)

    def contract(block, groups, fresh):
        cols = span(block, depth)

        def work(full):
            for kind, ref, act in ((0, pre, xa), (1, pre_down, ca)):
                lhs = weights(full, kind, cols)
                rows = slice(0, lhs.shape[0])
                for group in groups:
                    at = tokens_of(*group)
                    part = lax.dot_general(lhs, act[at, cols], last, preferred_element_type=f32)
                    ref[rows, at] = part if fresh else ref[rows, at] + part

        by_place(work)

    sides = peers(rep, n_rep)
    soon = [(side, False) for side in sides + [rep]]
    late = []
    for side in sides + [rep]:
        acts_arrived(side, home)
    if away:
        acts_arrived(rep, away)
        soon.append((rep, True))
        late = [(side, True) for side in sides]
    blocks = []
    for k in range(n_z):
        if k == n_z // 2:
            for other in away:
                from_rep(other)
        blocks.append(at_z(near[k]))
        contract(blocks[-1], soon, k == 0)
        for row in peers(y, n_y):
            blocks.append(at_z(near[k], row))
            for part in parts:
                w_arrived(part, blocks[-1])
            contract(blocks[-1], soon, False)
    out.finish()

    def activate(group):
        cols = tokens_of(*group)

        def rows_of(start, size, down):
            @pl.loop(0, size // 16)
            def _(step):
                gate = pl.ds(pl.multiple_of(start + step * 16, 16), 16)
                up = pl.ds(pl.multiple_of(start + size + step * 16, 16), 16)
                rows = pl.ds(pl.multiple_of(down + step * 16, 16), 16)
                gate_pre, up_pre, grad_hidden = pre[gate, cols], pre[up, cols], pre_down[rows, cols]
                sigmoid_gate = jax.nn.sigmoid(gate_pre)
                activated = gate_pre * sigmoid_gate
                ht[rows, cols] = (activated * up_pre).astype(bf16)
                gt[gate, cols] = (
                    grad_hidden * up_pre * sigmoid_gate * (1.0 + gate_pre * (1.0 - sigmoid_gate))
                ).astype(bf16)
                gt[up, cols] = (grad_hidden * activated).astype(bf16)

        rows_of(0, base, 0)
        if more:
            pl.when(inner)(lambda: rows_of(2 * base, more, base))

    def partial_inputs(group):
        rows = tokens_of(*group)

        def work(full):
            rhs = weights(full, 0, slice(None))
            p[rows] = lax.dot_general(
                gt[: rhs.shape[0], rows], rhs, first, preferred_element_type=f32
            ).astype(bf16)

        by_place(work)
        for other in away if group[1] else home[1:] + home[:1]:
            shard = group[0] * n_z + other
            for j in range(1, n_tp):
                peer = lax.rem(tp + j, n_tp)
                out.send(
                    p.at[span(shard, tokens), span(peer, width)],
                    p_in.at[j - 1, shard],
                    p_recv.at[j - 1, shard],
                    "tp",
                    peer,
                )

    def pair_wait(shard):
        for j in range(n_tp - 1):
            arrived(p_in.at[j, shard], p_recv.at[j, shard])

    def pair_sum(shard):
        value = p[span(shard, tokens), span(tp, width)].astype(f32)
        for j in range(n_tp - 1):
            value = value + p_in[j, shard].astype(f32)
        return value

    def weight_block(block, dst, dst_more):
        cols = span(block, depth)

        def work(full):
            held = units if full else base
            both = jnp.dot(gt[: 2 * held], xa[:, cols], preferred_element_type=f32)
            down = jnp.dot(ht[:held], ca[:, cols], preferred_element_type=f32)
            dst[: 2 * base] = both[: 2 * base].astype(dst.dtype)
            dst[2 * base :] = down[:base].astype(dst.dtype)
            if full:
                dst_more[: 2 * more] = both[2 * base :].astype(dst.dtype)
                dst_more[2 * more :] = down[base:].astype(dst.dtype)

        by_place(work)

    paired = n_z == 4
    if paired:
        taken = jnp.where(inside(z), away[0], away[1])
        given = jnp.where(inside(z), away[1], away[0])

    def rep_sum(other, from_sides=True):
        value = pair_sum(rep * n_z + other)
        for j in range(n_rep - 1 if from_sides else 0):
            value = value + x_in[j, other].astype(f32)
        return value

    def rep_wait(other):
        for j in range(n_rep - 1):
            arrived(x_in.at[j, other], x_recv.at[j, other])

    def toward(i, passing):
        other = others[i]
        from_sides = not paired or i == 2 or passing == (i == 0)
        up = other > z
        came = jnp.where(up, 0, 1)
        behind = jnp.where(up, z >= 1, z + 1 < n_z)
        when = behind if passing else jnp.logical_not(behind)
        slot, recv_sem = z_in.at[came, other], z_recv.at[came, other]

        @pl.when(when)
        def _():
            if from_sides:
                rep_wait(other)
            value = rep_sum(other, from_sides)
            if passing:
                arrived(slot, recv_sem)
                value = value + slot[...].astype(f32)
            r[other] = value.astype(bf16)

        peer = jnp.where(up, fs + n_y, fs - n_y)
        out.send(r.at[other], slot, recv_sem, "fs", peer, when)

    sets = [(gp, go, g_in, gs, dw)]
    if more:
        sets.append((gp_more, go_more, g_in_more, gs_more, dw_more))

    def dw_slot(extra, side, other):
        if extra:
            other = jnp.clip(other - 1, 0, n_z - 3)
            return dw_more.at[side * (n_z - 2) + other]
        return dw.at[side * n_z + other]

    def dw_send(extra, other, when):
        slot = dw_slot(extra, rep, other)
        for peer in peers(rep, n_rep):
            out.send(slot, slot, d_recv.at[extra, rep, other], "rep", peer, when)

    def g_step(other, own):
        def work(extra):
            partial, total, came, summed, _ = sets[extra]
            total = total[other]
            for j in range(n_y - 1):
                arrived(came.at[j, other], g_recv.at[extra, j, other])
                total = total + came[j, other].astype(f32)
            if own:
                dw_slot(extra, rep, z)[...] = total.astype(bf16)
            else:
                summed[other] = total.astype(bf16)

        for extra in range(len(sets)):
            if extra:
                pl.when(inner)(lambda: work(1))
            else:
                work(0)
            if own:
                dw_send(extra, z, here_too[extra])
            else:
                out.send(
                    sets[extra][3].at[other], dw_slot(extra, rep, z), d_recv.at[extra, rep, z],
                    "fs", at_z(other), here_too[extra],
                )

    def g_forward(other):
        for extra in range(len(sets)):
            when = inside(other) if extra else None
            arrived(dw_slot(extra, rep, other), d_recv.at[extra, rep, other], when)
            dw_send(extra, other, when)

    def to_row(other):
        for j in range(1, n_y):
            row = lax.rem(y + j, n_y)
            at = (j - 1, other)
            weight_block(at_z(other, row), gp.at[at], gp_more.at[at])
            for extra, (partial, _, came, *_) in enumerate(sets):
                out.send(
                    partial.at[at], came.at[at], g_recv.at[extra, j - 1, other],
                    "fs", at_z(z, row), here_too[extra],
                )

    def to_side(other, only=None):
        for j in range(1, n_rep):
            side = lax.rem(rep + j, n_rep)

            def work(j=j, side=side):
                if only is None:
                    pair_wait(side * n_z + other)
                value = pair_sum(side * n_z + other)
                if only is not None:
                    arrived(h_in.at[j - 1], h_recv.at[j - 1])
                    value = value + h_in[j - 1].astype(f32)
                q[j - 1, other] = value.astype(bf16)

            if only is None:
                work()
            else:
                pl.when(only)(work)
            out.send(
                q.at[j - 1, other], x_in.at[j - 1, other], x_recv.at[j - 1, other],
                "rep", side, only,
            )

    def give():
        for j in range(1, n_rep):
            side = lax.rem(rep + j, n_rep)
            for other in away:
                pair_wait(side * n_z + other)
            h[j - 1] = pair_sum(side * n_z + given).astype(bf16)
            out.send(h.at[j - 1], h_in.at[j - 1], h_recv.at[j - 1], "fs", at_z(home[1]))

    for group in soon[: len(sides)]:
        activate(group)
        partial_inputs(group)
    for group in soon[len(sides) :]:
        activate(group)
    for side, _ in late:
        acts_arrived(side, away)
    for i, block in enumerate(blocks if late else ()):
        contract(block, late, i == 0)
    for group in late:
        activate(group)
    rows = others[:-1] + [z] + others[-1:]
    to_row(rows[0])
    for other in home[1:]:
        to_side(other)
    for group in late:
        partial_inputs(group)
    if paired:
        to_side(z)
        give()
    for other in [] if paired else away + [z]:
        to_side(other)
    for other in rows[1:]:
        to_row(other)
    for group in soon[len(sides) :]:
        partial_inputs(group)
    for other in rows:
        weight_block(at_z(other), go.at[other], go_more.at[other])
    for other in far_first:
        pair_wait(rep * n_z + other)

    count = len(others)
    if paired:
        toward(0, False)
    for i, other in enumerate(others[:-1]):
        g_step(other, False)
        if paired:
            to_side(taken, inside(z) if i == 0 else jnp.logical_not(inside(z)))
        elif i == 0:
            toward(0, False)
    if count == 1:
        toward(0, False)
    if count:
        toward(0, True)
    g_step(z, True)
    for other in others[-1:]:
        g_step(other, False)
    if count > 1:
        g_forward(others[1])
        toward(1, False)
    for i in range(2, count):
        toward(i, False)
    for other in others[:1]:
        g_forward(other)
    if count > 1:
        toward(count - 1, True)
    for other in others[2:]:
        g_forward(other)
    for i in range(1, count - 1):
        toward(i, True)
    rep_wait(z)
    total[...] = rep_sum(z)
    for came, here in ((0, z >= 1), (1, z + 1 < n_z)):

        @pl.when(here)
        def _(came=came):
            arrived(z_in.at[came, z], z_recv.at[came, z])
            total[...] = total[...] + z_in[came, z].astype(f32)

    dx_ref[...] = total[...].astype(bf16)
    for side in peers(rep, n_rep):
        for other in [z] + others:
            for extra in range(len(sets)):
                arrived(
                    dw_slot(extra, side, other), d_recv.at[extra, side, other],
                    inside(other) if extra else None,
                )

    def gathered_rows(kind):
        rows = []
        for side in range(n_rep):
            for other in range(n_z):
                rows.append(dw[side * n_z + other, kind * base : (kind + 1) * base])
                if more and 0 < other < n_z - 1:
                    at = side * (n_z - 2) + other - 1
                    rows.append(dw_more[at, kind * more : (kind + 1) * more])
        return jnp.concatenate(rows, axis=0)

    dgate_ref[...] = gathered_rows(0).T
    dup_ref[...] = gathered_rows(1).T
    ddown_ref[...] = gathered_rows(2)
    out.finish()


VMEM = pl.BlockSpec(memory_space=pltpu.VMEM)
ANY = pl.BlockSpec(memory_space=pl.ANY)
DMA = pltpu.SemaphoreType.DMA


def widen_kernel(*refs):
    for src, dst in zip(refs[:4], refs[4:]):
        dst[...] = src[...].astype(dst.dtype)


def fused(sizes, x, c, gate_weight, up_weight, down_weight):
    bf16, f32 = jnp.bfloat16, jnp.float32
    n_rep, n_fs, n_tp, n_y = sizes
    n_z = n_fs // n_y
    tokens, width = x.shape
    depth, hidden_tp = gate_weight.shape
    model, per_rep = width * n_tp, hidden_tp // n_rep
    base, more = per_rep // n_z, 0
    for size in range(16, per_rep, 16) if n_z > 2 else ():
        rest = per_rep - (n_z - 2) * size
        if rest % (16 * n_z) == 0 and 4 * size * n_z <= 3 * rest:
            base, more = rest // n_z, size
    units, spare, mids = base + more, max(more, 16), max(n_z - 2, 1)
    kinds = 4 if more else 2
    shards = n_rep * n_z
    group = shards * tokens
    tp_rep = n_tp + n_rep - 2
    n_sends = (
        2 * (2 + tp_rep) + 4 * ((n_z - 1) * (1 + tp_rep) - 1) + 2 * (n_z + n_z // 2) * (n_rep - 1) * (n_tp - 1)
        + kinds * (n_y - 1) * n_z + 2 * kinds * (n_z - 1 + (n_z > 3))
    )
    grad_inputs, *grads = pl.pallas_call(
        functools.partial(layer_kernel, sizes),
        out_shape=(
            jax.ShapeDtypeStruct((tokens, width), bf16),
            jax.ShapeDtypeStruct((depth, hidden_tp), bf16),
            jax.ShapeDtypeStruct((depth, hidden_tp), bf16),
            jax.ShapeDtypeStruct((hidden_tp, depth), bf16),
        ),
        in_specs=[ANY] * 5,
        out_specs=(VMEM,) * 4,
        scratch_shapes=[
            *(pltpu.VMEM(v.shape, bf16) for v in (x, c, gate_weight, up_weight, down_weight)),
            DMA((5,)),
            pltpu.VMEM((group, model), bf16),
            pltpu.VMEM((group, model), bf16),
            pltpu.VMEM((2, hidden_tp, depth), bf16),
            pltpu.VMEM((3, base, model), bf16),
            pltpu.VMEM((3, spare, model), bf16),
            pltpu.VMEM((2 * units, group), f32),
            pltpu.VMEM((units, group), f32),
            pltpu.VMEM((2 * units, group), bf16),
            pltpu.VMEM((units, group), bf16),
            pltpu.VMEM((group, model), bf16),
            pltpu.VMEM((n_tp - 1, shards, tokens, width), bf16),
            pltpu.VMEM((n_rep - 1, n_z, tokens, width), bf16),
            pltpu.VMEM((n_rep - 1, n_z, tokens, width), bf16),
            pltpu.VMEM((n_z, tokens, width), bf16),
            pltpu.VMEM((2, n_z, tokens, width), bf16),
            pltpu.VMEM((tokens, width), f32),
            pltpu.VMEM((n_rep - 1, tokens, width), bf16),
            pltpu.VMEM((n_rep - 1, tokens, width), bf16),
            *(
                pltpu.VMEM((*lead, 3 * size, depth), kind)
                for size, places in ((base, shards), (spare, n_rep * mids))
                for lead, kind in (
                    ((n_y - 1, n_z), bf16), ((n_z,), f32), ((n_y - 1, n_z), bf16),
                    ((n_z,), bf16), ((places,), bf16),
                )
            ),
            DMA((n_sends,)),
            DMA((2, shards, n_tp)),
            DMA((kinds, n_fs)),
            DMA((n_tp - 1, shards)),
            DMA((n_rep - 1, n_z)),
            DMA((2, n_z)),
            DMA((kinds // 2, n_y - 1, n_z)),
            DMA((kinds // 2, n_rep, n_z)),
            DMA((n_rep - 1,)),
        ],
        compiler_params=pltpu.CompilerParams(
            collective_id=0, has_side_effects=True, vmem_limit_bytes=60 * 2**20
        ),
    )(x, c, gate_weight, up_weight, down_weight)
    steps = 2

    def block(shape):
        return pl.BlockSpec((shape[0] // steps, shape[1]), lambda i: (i, 0))

    results = (grad_inputs, *grads)
    return pl.pallas_call(
        widen_kernel,
        grid=(steps,),
        out_shape=[
            jax.ShapeDtypeStruct(v.shape, f32 if i else bf16) for i, v in enumerate(results)
        ],
        in_specs=[block(v.shape) for v in results],
        out_specs=[block(v.shape) for v in results],
    )(*results)


def gathered(x, c, gate_weight, up_weight, down_weight):
    bf16, f32 = jnp.bfloat16, jnp.float32
    last = (((1,), (1,)), ((), ()))
    first = (((0,), (0,)), ((), ()))
    x, c = (lax.all_gather(v, "tp", axis=1, tiled=True) for v in (x, c))
    gate, up = (lax.all_gather(v, "fs", axis=0, tiled=True) for v in (gate_weight, up_weight))
    down = lax.all_gather(down_weight, "fs", axis=1, tiled=True)
    gate_pre = jnp.dot(x, gate, preferred_element_type=f32)
    up_pre = jnp.dot(x, up, preferred_element_type=f32)
    grad_hidden = lax.dot_general(c, down, last, preferred_element_type=f32)
    sigmoid_gate = jax.nn.sigmoid(gate_pre)
    activated = gate_pre * sigmoid_gate
    hidden = (activated * up_pre).astype(bf16)
    grad_gate = (
        grad_hidden * up_pre * sigmoid_gate * (1.0 + gate_pre * (1.0 - sigmoid_gate))
    ).astype(bf16)
    grad_up = (grad_hidden * activated).astype(bf16)
    partial_sum = lax.dot_general(grad_gate, gate, last, preferred_element_type=f32)
    partial_sum += lax.dot_general(grad_up, up, last, preferred_element_type=f32)
    grad_inputs = lax.psum_scatter(partial_sum, "tp", scatter_dimension=1, tiled=True)

    def scattered(lhs, rhs, dimension):
        grads = lax.dot_general(lhs, rhs, first, preferred_element_type=f32)
        grads = lax.psum_scatter(grads, "fs", scatter_dimension=dimension, tiled=True)
        return lax.psum(grads, "rep")

    return (
        grad_inputs.astype(bf16),
        scattered(x, grad_gate, 0),
        scattered(x, grad_up, 0),
        scattered(hidden, c, 1),
    )


def per_device(n_rep, n_fs, n_tp, x, c, gate_weight, up_weight, down_weight):
    n_y = max(k for k in range(1, n_fs + 1) if n_fs % k == 0 and k * k <= n_fs)
    n_z = n_fs // n_y
    tokens, width = x.shape
    depth, hidden_tp = gate_weight.shape
    args = (x, c, gate_weight, up_weight, down_weight)
    whole = hidden_tp % (16 * n_rep * n_z) == 0
    if whole and tokens % 128 == width % 128 == depth % 128 == 0 and min(n_rep, n_y, n_tp) > 1:
        return fused((n_rep, n_fs, n_tp, n_y), *args)
    return gathered(*args)


def solution(mesh):
    n_rep, n_fs, n_tp = (mesh.shape[axis] for axis in ("rep", "fs", "tp"))
    placed = (
        P(("rep", "fs"), "tp"),
        P(("rep", "fs"), "tp"),
        P("fs", "tp"),
        P("fs", "tp"),
        P("tp", "fs"),
    )
    return jax.shard_map(
        functools.partial(per_device, n_rep, n_fs, n_tp),
        mesh=mesh,
        in_specs=placed,
        out_specs=(P(("rep", "fs"), "tp"), P("fs", "tp"), P("fs", "tp"), P("tp", "fs")),
        check_vma=False,
    )
```

```python
import functools

import jax
import jax.numpy as jnp
from jax import lax
from jax.experimental import pallas as pl
from jax.experimental.pallas import tpu as pltpu
from jax.sharding import PartitionSpec as P

MESH = pl.DeviceIdType.MESH


def greet(n_rep, n_fs, n_tp):
    barrier = pltpu.get_barrier_semaphore()
    for axis, n in (("rep", n_rep), ("fs", n_fs), ("tp", n_tp)):
        me = lax.axis_index(axis)
        for k in range(1, n):
            pl.semaphore_signal(
                barrier, inc=1, device_id={axis: lax.rem(me + k, n)}, device_id_type=MESH
            )
    return lambda: pl.semaphore_wait(barrier, n_rep + n_fs + n_tp - 3)


class Sender:
    def __init__(self, sems):
        self.sems, self.used, self.pending = sems, 0, []

    def run(self, build, when):
        if when is None:
            build().start()
        else:
            pl.when(when)(lambda: build().start())

    def send(self, src, dst, recv_sem, axis, peer, when=None):
        def build(at=self.used):
            return pltpu.make_async_remote_copy(
                src_ref=src,
                dst_ref=dst,
                send_sem=self.sems.at[at],
                recv_sem=recv_sem,
                device_id={axis: peer},
                device_id_type=MESH,
            )

        self.used += 1
        self.run(build, when)
        self.pending.append((lambda: build().wait_send(), when))

    def local(self, src, dst):
        def build(at=self.used):
            return pltpu.make_async_copy(src, dst, self.sems.at[at])

        self.used += 1
        self.run(build, None)
        self.pending.append((lambda: build().wait(), None))

    def finish(self):
        for wait, when in self.pending:
            if when is None:
                wait()
            else:
                pl.when(when)(wait)
        self.used, self.pending = 0, []


def arrived(slot, recv_sem, when=None):
    def wait():
        pltpu.make_async_copy(slot, slot, recv_sem).wait()

    if when is None:
        wait()
    else:
        pl.when(when)(wait)


def near_first(n):
    return sorted(range(1, n), key=lambda k: min(k, n - k))


def layer_kernel(
    sizes, *refs
):
    inputs, rest = refs[:5], refs[5:]
    outputs, local, loads, rest = rest[:4], rest[4:9], rest[9], rest[10:]
    met = greet(*sizes[:3])
    copies = [pltpu.make_async_copy(a, b, loads.at[i]) for i, (a, b) in enumerate(zip(inputs, local))]
    for copy in copies:
        copy.start()
    met()
    layer(sizes, copies, *local, *outputs, *rest)


def layer(
    sizes, copies, x_ref, c_ref, gate_ref, up_ref, down_ref, dx_ref, dgate_ref, dup_ref, ddown_ref,
    xa, ca, wt, wa, wa_more, pre, pre_down, gt, ht,
    p, p_in, q, x_in, r, z_in, total, h, h_in,
    gp, go, g_in, gs, dw, gp_more, go_more, g_in_more, gs_more, dw_more,
    sends, act_recv, w_recv, p_recv, x_recv, z_recv, g_recv, d_recv, h_recv,
):
    n_rep, n_fs, n_tp, n_y = sizes
    n_z = n_fs // n_y
    f32, bf16 = jnp.float32, jnp.bfloat16
    rep, fs, tp = (lax.axis_index(axis) for axis in ("rep", "fs", "tp"))
    z, y = fs // n_y, lax.rem(fs, n_y)
    tokens, width = x_ref.shape
    base, more, depth = wa.shape[1], ht.shape[0] - wa.shape[1], down_ref.shape[1]
    units = base + more
    inner = jnp.logical_and(z > 0, z < n_z - 1) if more else None
    out = Sender(sends)

    def span(at, size):
        return pl.ds(pl.multiple_of(at * size, size), size)

    def peers(me, n):
        return [lax.rem(me + k, n) for k in range(1, n)]

    def at_z(other, row=y):
        return other * n_y + row

    far_first, low, high = [], 0, n_z - 1
    for _ in range(n_z):
        above = 2 * (high - z) + jnp.where(2 * z < n_z, 1, 0) > 2 * (z - low)
        far_first.append(jnp.where(above, high, low))
        low, high = jnp.where(above, low, low + 1), jnp.where(above, high - 1, high)
    others = far_first[:-1]
    near = [z] + others[::-1]
    halves = 1 if n_z % 2 else 2
    half = n_z // halves
    start = z // half * half
    home = [start + lax.rem(z - start + i, half) for i in range(half)]
    away = [jnp.where(z < half, n_z - 1 - i, i) for i in range(n_z - half)]

    own_acts, acts = (x_ref, c_ref), (xa, ca)

    def act_slot(a, shard, part):
        return acts[a].at[span(shard, tokens), span(part, width)]

    def act_send(a, shard, src, axis, peer, when=None):
        out.send(src, act_slot(a, shard, tp), act_recv.at[a, shard, tp], axis, peer, when)

    def to_rep(a, shard, src, when=None):
        for peer in peers(rep, n_rep):
            act_send(a, shard, src, "rep", peer, when)

    def to_tp(a, shard, src, when=None):
        for peer in peers(tp, n_tp):
            act_send(a, shard, src, "tp", peer, when)

    def from_rep(other, only=None):
        for peer in peers(rep, n_rep):
            for a in range(2):
                shard = peer * n_z + other
                slot = act_slot(a, shard, tp)
                arrived(slot, act_recv.at[a, shard, tp], only)
                to_tp(a, shard, slot, only)

    mine = rep * n_z + z
    for a in range(2):
        copies[a].wait()
        act_send(a, mine, own_acts[a], "fs", fs + n_y, z + 1 < n_z)
        act_send(a, mine, own_acts[a], "fs", fs - n_y, z >= 1)
        to_rep(a, mine, own_acts[a])
    for a in range(2):
        to_tp(a, mine, own_acts[a])

    for copy in copies[2:]:
        copy.wait()
    wt[0] = gate_ref[...].T
    wt[1] = up_ref[...].T

    def inside(other):
        return jnp.logical_and(other > 0, other < n_z - 1)

    parts = [(0, 0), (0, 1), (1, 0), (1, 1)][: 4 if more else 2]
    here_too = {0: None, 1: inner}

    def w_part(extra, kind, other):
        start = rep * (n_z * base + max(n_z - 2, 0) * more) + other * units
        start = start - (jnp.minimum(other, 1) * more if more else 0) + extra * base
        rows = pl.ds(pl.multiple_of(start, 16), more if extra else base)
        return down_ref.at[rows] if kind else wt.at[:, rows]

    def w_slot(extra, kind, block):
        held = wa_more if extra else wa
        return held.at[2 if kind else slice(0, 2), :, span(block, depth)]

    def w_send(part, block, src, peer, when=None):
        out.send(src, w_slot(*part, block), w_recv.at[parts.index(part), block], "fs", peer, when)

    def w_arrived(part, block):
        arrived(w_slot(*part, block), w_recv.at[parts.index(part), block], here_too[part[0]])

    for part in parts:
        for row in peers(y, n_y):
            w_send(part, fs, w_part(*part, z), at_z(z, row), here_too[part[0]])

    def keep(part):
        held, (extra, kind) = (wa_more if part[0] else wa), part
        if kind:
            held[2, :, span(fs, depth)] = w_part(*part, z)[...]
        else:
            held[0:2, :, span(fs, depth)] = w_part(*part, z)[...]

    for part in parts:
        if part[0]:
            pl.when(inner)(functools.partial(keep, part))
        else:
            keep(part)
    for a in range(2):
        acts[a][span(mine, tokens), span(tp, width)] = own_acts[a][...]

    def send_weights(step, only=None):
        ways = [(1, z + step < n_z), (-1, z >= step)]
        if 2 * step >= n_z:
            ways = [(jnp.where(ways[0][1], 1, -1), jnp.logical_or(ways[0][1], ways[1][1]))]
        for sign, here in ways:
            other = z + sign * step
            here = here if only is None else jnp.logical_and(here, only)
            for part in parts:
                when = jnp.logical_and(here, inside(other)) if part[0] else here
                w_send(part, fs, w_part(*part, other), at_z(other), when)

    def swap_weights(other):
        for part in parts:
            block = at_z(other)
            w_arrived(part, block)
            for row in peers(y, n_y):
                w_send(part, block, w_slot(*part, block), at_z(z, row), here_too[part[0]])

    held = n_z > 3
    for k in range(1, n_z):
        for a in range(2):
            ways = [(z >= k, z + 1 < n_z, -1), (z + k < n_z, z >= 1, 1)]
            if 2 * k >= n_z:
                up = z >= k
                here, onward = jnp.logical_or(up, z + k < n_z), jnp.where(up, z + 1, n_z - z) < n_z
                ways = [(here, onward, jnp.where(up, -1, 1))]
            for here, onward, step in ways:
                shard = mine + step * k
                slot = act_slot(a, shard, tp)
                arrived(slot, act_recv.at[a, shard, tp], here)
                if k < n_z - 1:
                    act_send(a, shard, slot, "fs", fs - step * n_y, jnp.logical_and(here, onward))
                to_rep(a, shard, slot, here)
                to_tp(a, shard, slot, here)
            if k == n_z - 1 and a == 0:
                send_weights(k)
                for other in home[1:]:
                    from_rep(other, jnp.logical_not(inside(z)) if held else None)
        if k < n_z - 2 or not held and k == n_z - 2:
            send_weights(k)
        if k == 1:
            from_rep(z)
        if held and k == n_z - 2:
            send_weights(k, jnp.logical_not(inside(z)))
            swap_weights(near[1])
    if n_z == 1:
        from_rep(z)
    if held:
        near[2], near[3] = near[3], near[2]
        swap_weights(near[2])
        for other in home[1:]:
            from_rep(other, inside(z))
        swap_weights(near[3])
        send_weights(n_z - 2, inside(z))
    for k in range(4 if held else 1, n_z):
        swap_weights(near[k])
    def acts_arrived(side, places):
        for part in peers(tp, n_tp):
            for other in places:
                for a in range(2):
                    shard = side * n_z + other
                    arrived(act_slot(a, shard, part), act_recv.at[a, shard, part])

    last = (((1,), (1,)), ((), ()))
    first = (((0,), (0,)), ((), ()))

    def by_place(work):
        if not more:
            work(False)
        else:
            pl.when(inner)(lambda: work(True))
            pl.when(jnp.logical_not(inner))(lambda: work(False))

    def weights(full, kind, cols):
        rows = slice(2, 3) if kind else slice(0, 2)
        value = wa[rows, :, cols]
        value = value.reshape(-1, value.shape[-1])
        if full:
            extra = wa_more[rows, :, cols]
            value = jnp.concatenate([value, extra.reshape(-1, value.shape[-1])], axis=0)
        return value

    def tokens_of(side, away):
        place = z // half
        return span(side * halves + (1 - place if away else place), half * tokens)

    def contract(block, groups, fresh):
        cols = span(block, depth)

        def work(full):
            for kind, ref, act in ((0, pre, xa), (1, pre_down, ca)):
                lhs = weights(full, kind, cols)
                rows = slice(0, lhs.shape[0])
                for group in groups:
                    at = tokens_of(*group)
                    part = lax.dot_general(lhs, act[at, cols], last, preferred_element_type=f32)
                    ref[rows, at] = part if fresh else ref[rows, at] + part

        by_place(work)

    sides = peers(rep, n_rep)
    soon = [(side, False) for side in sides + [rep]]
    late = []
    for side in sides + [rep]:
        acts_arrived(side, home)
    if away:
        acts_arrived(rep, away)
        soon.append((rep, True))
        late = [(side, True) for side in sides]
    blocks = []
    for k in range(n_z):
        if k == n_z // 2:
            for other in away:
                from_rep(other)
        blocks.append(at_z(near[k]))
        contract(blocks[-1], soon, k == 0)
        for row in peers(y, n_y):
            blocks.append(at_z(near[k], row))
            for part in parts:
                w_arrived(part, blocks[-1])
            contract(blocks[-1], soon, False)
    out.finish()

    def activate(group):
        cols = tokens_of(*group)

        def rows_of(start, size, down):
            @pl.loop(0, size // 16)
            def _(step):
                gate = pl.ds(pl.multiple_of(start + step * 16, 16), 16)
                up = pl.ds(pl.multiple_of(start + size + step * 16, 16), 16)
                rows = pl.ds(pl.multiple_of(down + step * 16, 16), 16)
                gate_pre, up_pre, grad_hidden = pre[gate, cols], pre[up, cols], pre_down[rows, cols]
                sigmoid_gate = jax.nn.sigmoid(gate_pre)
                activated = gate_pre * sigmoid_gate
                ht[rows, cols] = (activated * up_pre).astype(bf16)
                gt[gate, cols] = (
                    grad_hidden * up_pre * sigmoid_gate * (1.0 + gate_pre * (1.0 - sigmoid_gate))
                ).astype(bf16)
                gt[up, cols] = (grad_hidden * activated).astype(bf16)

        rows_of(0, base, 0)
        if more:
            pl.when(inner)(lambda: rows_of(2 * base, more, base))

    def partial_inputs(group):
        rows = tokens_of(*group)

        def work(full):
            rhs = weights(full, 0, slice(None))
            p[rows] = lax.dot_general(
                gt[: rhs.shape[0], rows], rhs, first, preferred_element_type=f32
            ).astype(bf16)

        by_place(work)
        for other in away if group[1] else home[1:] + home[:1]:
            shard = group[0] * n_z + other
            for j in range(1, n_tp):
                peer = lax.rem(tp + j, n_tp)
                out.send(
                    p.at[span(shard, tokens), span(peer, width)],
                    p_in.at[j - 1, shard],
                    p_recv.at[j - 1, shard],
                    "tp",
                    peer,
                )

    def pair_wait(shard):
        for j in range(n_tp - 1):
            arrived(p_in.at[j, shard], p_recv.at[j, shard])

    def pair_sum(shard):
        value = p[span(shard, tokens), span(tp, width)].astype(f32)
        for j in range(n_tp - 1):
            value = value + p_in[j, shard].astype(f32)
        return value

    def weight_block(block, dst, dst_more):
        cols = span(block, depth)

        def work(full):
            held = units if full else base
            both = jnp.dot(gt[: 2 * held], xa[:, cols], preferred_element_type=f32)
            down = jnp.dot(ht[:held], ca[:, cols], preferred_element_type=f32)
            dst[: 2 * base] = both[: 2 * base].astype(dst.dtype)
            dst[2 * base :] = down[:base].astype(dst.dtype)
            if full:
                dst_more[: 2 * more] = both[2 * base :].astype(dst.dtype)
                dst_more[2 * more :] = down[base:].astype(dst.dtype)

        by_place(work)

    paired = n_z == 4
    if paired:
        taken = jnp.where(inside(z), away[0], away[1])
        given = jnp.where(inside(z), away[1], away[0])

    def rep_sum(other, from_sides=True):
        value = pair_sum(rep * n_z + other)
        for j in range(n_rep - 1 if from_sides else 0):
            value = value + x_in[j, other].astype(f32)
        return value

    def rep_wait(other):
        for j in range(n_rep - 1):
            arrived(x_in.at[j, other], x_recv.at[j, other])

    def toward(i, passing):
        other = others[i]
        from_sides = not paired or i == 2 or passing == (i == 0)
        up = other > z
        came = jnp.where(up, 0, 1)
        behind = jnp.where(up, z >= 1, z + 1 < n_z)
        when = behind if passing else jnp.logical_not(behind)
        slot, recv_sem = z_in.at[came, other], z_recv.at[came, other]

        @pl.when(when)
        def _():
            if from_sides:
                rep_wait(other)
            value = rep_sum(other, from_sides)
            if passing:
                arrived(slot, recv_sem)
                value = value + slot[...].astype(f32)
            r[other] = value.astype(bf16)

        peer = jnp.where(up, fs + n_y, fs - n_y)
        out.send(r.at[other], slot, recv_sem, "fs", peer, when)

    sets = [(gp, go, g_in, gs, dw)]
    if more:
        sets.append((gp_more, go_more, g_in_more, gs_more, dw_more))

    def dw_slot(extra, side, other):
        if extra:
            other = jnp.clip(other - 1, 0, n_z - 3)
            return dw_more.at[side * (n_z - 2) + other]
        return dw.at[side * n_z + other]

    def dw_send(extra, other, when):
        slot = dw_slot(extra, rep, other)
        for peer in peers(rep, n_rep):
            out.send(slot, slot, d_recv.at[extra, rep, other], "rep", peer, when)

    def g_step(other, own):
        def work(extra):
            partial, total, came, summed, _ = sets[extra]
            total = total[other]
            for j in range(n_y - 1):
                arrived(came.at[j, other], g_recv.at[extra, j, other])
                total = total + came[j, other].astype(f32)
            if own:
                dw_slot(extra, rep, z)[...] = total.astype(bf16)
            else:
                summed[other] = total.astype(bf16)

        for extra in range(len(sets)):
            if extra:
                pl.when(inner)(lambda: work(1))
            else:
                work(0)
            if own:
                dw_send(extra, z, here_too[extra])
            else:
                out.send(
                    sets[extra][3].at[other], dw_slot(extra, rep, z), d_recv.at[extra, rep, z],
                    "fs", at_z(other), here_too[extra],
                )

    def g_forward(other):
        for extra in range(len(sets)):
            when = inside(other) if extra else None
            arrived(dw_slot(extra, rep, other), d_recv.at[extra, rep, other], when)
            dw_send(extra, other, when)

    def to_row(other):
        for j in range(1, n_y):
            row = lax.rem(y + j, n_y)
            at = (j - 1, other)
            weight_block(at_z(other, row), gp.at[at], gp_more.at[at])
            for extra, (partial, _, came, *_) in enumerate(sets):
                out.send(
                    partial.at[at], came.at[at], g_recv.at[extra, j - 1, other],
                    "fs", at_z(z, row), here_too[extra],
                )

    def to_side(other, only=None):
        for j in range(1, n_rep):
            side = lax.rem(rep + j, n_rep)

            def work(j=j, side=side):
                if only is None:
                    pair_wait(side * n_z + other)
                value = pair_sum(side * n_z + other)
                if only is not None:
                    arrived(h_in.at[j - 1], h_recv.at[j - 1])
                    value = value + h_in[j - 1].astype(f32)
                q[j - 1, other] = value.astype(bf16)

            if only is None:
                work()
            else:
                pl.when(only)(work)
            out.send(
                q.at[j - 1, other], x_in.at[j - 1, other], x_recv.at[j - 1, other],
                "rep", side, only,
            )

    def give():
        for j in range(1, n_rep):
            side = lax.rem(rep + j, n_rep)
            for other in away:
                pair_wait(side * n_z + other)
            h[j - 1] = pair_sum(side * n_z + given).astype(bf16)
            out.send(h.at[j - 1], h_in.at[j - 1], h_recv.at[j - 1], "fs", at_z(home[1]))

    for group in soon[: len(sides)]:
        activate(group)
        partial_inputs(group)
    for group in soon[len(sides) :]:
        activate(group)
    for side, _ in late:
        acts_arrived(side, away)
    for i, block in enumerate(blocks if late else ()):
        contract(block, late, i == 0)
    for group in late:
        activate(group)
    rows = others[:-1] + [z] + others[-1:]
    to_row(rows[0])
    for other in home[1:]:
        to_side(other)
    for group in late:
        partial_inputs(group)
    if paired:
        to_side(z)
        give()
    for other in [] if paired else away + [z]:
        to_side(other)
    for other in rows[1:]:
        to_row(other)
    for group in soon[len(sides) :]:
        partial_inputs(group)
    for other in rows:
        weight_block(at_z(other), go.at[other], go_more.at[other])
    for other in far_first:
        pair_wait(rep * n_z + other)

    count = len(others)
    if paired:
        toward(0, False)
    for i, other in enumerate(others[:-1]):
        g_step(other, False)
        if paired:
            to_side(taken, inside(z) if i == 0 else jnp.logical_not(inside(z)))
        elif i == 0:
            toward(0, False)
    if count == 1:
        toward(0, False)
    if count:
        toward(0, True)
    g_step(z, True)
    for other in others[-1:]:
        g_step(other, False)
    if count > 1:
        g_forward(others[1])
        toward(1, False)
    for i in range(2, count):
        toward(i, False)
    for other in others[:1]:
        g_forward(other)
    if count > 1:
        toward(count - 1, True)
    for other in others[2:]:
        g_forward(other)
    for i in range(1, count - 1):
        toward(i, True)
    rep_wait(z)
    total[...] = rep_sum(z)
    for came, here in ((0, z >= 1), (1, z + 1 < n_z)):

        @pl.when(here)
        def _(came=came):
            arrived(z_in.at[came, z], z_recv.at[came, z])
            total[...] = total[...] + z_in[came, z].astype(f32)

    dx_ref[...] = total[...].astype(bf16)
    for side in peers(rep, n_rep):
        for other in [z] + others:
            for extra in range(len(sets)):
                arrived(
                    dw_slot(extra, side, other), d_recv.at[extra, side, other],
                    inside(other) if extra else None,
                )

    def gathered_rows(kind):
        rows = []
        for side in range(n_rep):
            for other in range(n_z):
                rows.append(dw[side * n_z + other, kind * base : (kind + 1) * base])
                if more and 0 < other < n_z - 1:
                    at = side * (n_z - 2) + other - 1
                    rows.append(dw_more[at, kind * more : (kind + 1) * more])
        return jnp.concatenate(rows, axis=0)

    dgate_ref[...] = gathered_rows(0).T
    dup_ref[...] = gathered_rows(1).T
    ddown_ref[...] = gathered_rows(2)
    out.finish()


VMEM = pl.BlockSpec(memory_space=pltpu.VMEM)
ANY = pl.BlockSpec(memory_space=pl.ANY)
DMA = pltpu.SemaphoreType.DMA


def widen_kernel(*refs):
    for src, dst in zip(refs[:4], refs[4:]):
        dst[...] = src[...].astype(dst.dtype)


def fused(sizes, x, c, gate_weight, up_weight, down_weight):
    bf16, f32 = jnp.bfloat16, jnp.float32
    n_rep, n_fs, n_tp, n_y = sizes
    n_z = n_fs // n_y
    tokens, width = x.shape
    depth, hidden_tp = gate_weight.shape
    model, per_rep = width * n_tp, hidden_tp // n_rep
    base, more = per_rep // n_z, 0
    for size in range(16, per_rep, 16) if n_z > 2 else ():
        rest = per_rep - (n_z - 2) * size
        if rest % (16 * n_z) == 0 and 4 * size * n_z <= 3 * rest:
            base, more = rest // n_z, size
    units, spare, mids = base + more, max(more, 16), max(n_z - 2, 1)
    kinds = 4 if more else 2
    shards = n_rep * n_z
    group = shards * tokens
    tp_rep = n_tp + n_rep - 2
    ways = sum(2 - (2 * k >= n_z) for k in range(1, n_z))
    n_sends = (
        2 * (2 + tp_rep) + 2 * (ways * (1 + tp_rep) - 1) + 2 * (n_z + n_z // 2) * (n_rep - 1) * (n_tp - 1)
        + kinds * (n_y - 1) * n_z + kinds * (ways + (n_z > 3))
    )
    grad_inputs, *grads = pl.pallas_call(
        functools.partial(layer_kernel, sizes),
        out_shape=(
            jax.ShapeDtypeStruct((tokens, width), bf16),
            jax.ShapeDtypeStruct((depth, hidden_tp), bf16),
            jax.ShapeDtypeStruct((depth, hidden_tp), bf16),
            jax.ShapeDtypeStruct((hidden_tp, depth), bf16),
        ),
        in_specs=[ANY] * 5,
        out_specs=(VMEM,) * 4,
        scratch_shapes=[
            *(pltpu.VMEM(v.shape, bf16) for v in (x, c, gate_weight, up_weight, down_weight)),
            DMA((5,)),
            pltpu.VMEM((group, model), bf16),
            pltpu.VMEM((group, model), bf16),
            pltpu.VMEM((2, hidden_tp, depth), bf16),
            pltpu.VMEM((3, base, model), bf16),
            pltpu.VMEM((3, spare, model), bf16),
            pltpu.VMEM((2 * units, group), f32),
            pltpu.VMEM((units, group), f32),
            pltpu.VMEM((2 * units, group), bf16),
            pltpu.VMEM((units, group), bf16),
            pltpu.VMEM((group, model), bf16),
            pltpu.VMEM((n_tp - 1, shards, tokens, width), bf16),
            pltpu.VMEM((n_rep - 1, n_z, tokens, width), bf16),
            pltpu.VMEM((n_rep - 1, n_z, tokens, width), bf16),
            pltpu.VMEM((n_z, tokens, width), bf16),
            pltpu.VMEM((2, n_z, tokens, width), bf16),
            pltpu.VMEM((tokens, width), f32),
            pltpu.VMEM((n_rep - 1, tokens, width), bf16),
            pltpu.VMEM((n_rep - 1, tokens, width), bf16),
            *(
                pltpu.VMEM((*lead, 3 * size, depth), kind)
                for size, places in ((base, shards), (spare, n_rep * mids))
                for lead, kind in (
                    ((n_y - 1, n_z), bf16), ((n_z,), f32), ((n_y - 1, n_z), bf16),
                    ((n_z,), bf16), ((places,), bf16),
                )
            ),
            DMA((n_sends,)),
            DMA((2, shards, n_tp)),
            DMA((kinds, n_fs)),
            DMA((n_tp - 1, shards)),
            DMA((n_rep - 1, n_z)),
            DMA((2, n_z)),
            DMA((kinds // 2, n_y - 1, n_z)),
            DMA((kinds // 2, n_rep, n_z)),
            DMA((n_rep - 1,)),
        ],
        compiler_params=pltpu.CompilerParams(
            collective_id=0, has_side_effects=True, vmem_limit_bytes=60 * 2**20
        ),
    )(x, c, gate_weight, up_weight, down_weight)
    steps = 2

    def block(shape):
        return pl.BlockSpec((shape[0] // steps, shape[1]), lambda i: (i, 0))

    results = (grad_inputs, *grads)
    return pl.pallas_call(
        widen_kernel,
        grid=(steps,),
        out_shape=[
            jax.ShapeDtypeStruct(v.shape, f32 if i else bf16) for i, v in enumerate(results)
        ],
        in_specs=[block(v.shape) for v in results],
        out_specs=[block(v.shape) for v in results],
    )(*results)


def gathered(x, c, gate_weight, up_weight, down_weight):
    bf16, f32 = jnp.bfloat16, jnp.float32
    last = (((1,), (1,)), ((), ()))
    first = (((0,), (0,)), ((), ()))
    x, c = (lax.all_gather(v, "tp", axis=1, tiled=True) for v in (x, c))
    gate, up = (lax.all_gather(v, "fs", axis=0, tiled=True) for v in (gate_weight, up_weight))
    down = lax.all_gather(down_weight, "fs", axis=1, tiled=True)
    gate_pre = jnp.dot(x, gate, preferred_element_type=f32)
    up_pre = jnp.dot(x, up, preferred_element_type=f32)
    grad_hidden = lax.dot_general(c, down, last, preferred_element_type=f32)
    sigmoid_gate = jax.nn.sigmoid(gate_pre)
    activated = gate_pre * sigmoid_gate
    hidden = (activated * up_pre).astype(bf16)
    grad_gate = (
        grad_hidden * up_pre * sigmoid_gate * (1.0 + gate_pre * (1.0 - sigmoid_gate))
    ).astype(bf16)
    grad_up = (grad_hidden * activated).astype(bf16)
    partial_sum = lax.dot_general(grad_gate, gate, last, preferred_element_type=f32)
    partial_sum += lax.dot_general(grad_up, up, last, preferred_element_type=f32)
    grad_inputs = lax.psum_scatter(partial_sum, "tp", scatter_dimension=1, tiled=True)

    def scattered(lhs, rhs, dimension):
        grads = lax.dot_general(lhs, rhs, first, preferred_element_type=f32)
        grads = lax.psum_scatter(grads, "fs", scatter_dimension=dimension, tiled=True)
        return lax.psum(grads, "rep")

    return (
        grad_inputs.astype(bf16),
        scattered(x, grad_gate, 0),
        scattered(x, grad_up, 0),
        scattered(hidden, c, 1),
    )


def per_device(n_rep, n_fs, n_tp, x, c, gate_weight, up_weight, down_weight):
    n_y = max(k for k in range(1, n_fs + 1) if n_fs % k == 0 and k * k <= n_fs)
    n_z = n_fs // n_y
    tokens, width = x.shape
    depth, hidden_tp = gate_weight.shape
    args = (x, c, gate_weight, up_weight, down_weight)
    whole = hidden_tp % (16 * n_rep * n_z) == 0
    if whole and tokens % 128 == width % 128 == depth % 128 == 0 and min(n_rep, n_y, n_tp) > 1:
        return fused((n_rep, n_fs, n_tp, n_y), *args)
    return gathered(*args)


def solution(mesh):
    n_rep, n_fs, n_tp = (mesh.shape[axis] for axis in ("rep", "fs", "tp"))
    placed = (
        P(("rep", "fs"), "tp"),
        P(("rep", "fs"), "tp"),
        P("fs", "tp"),
        P("fs", "tp"),
        P("tp", "fs"),
    )
    return jax.shard_map(
        functools.partial(per_device, n_rep, n_fs, n_tp),
        mesh=mesh,
        in_specs=placed,
        out_specs=(P(("rep", "fs"), "tp"), P("fs", "tp"), P("fs", "tp"), P("tp", "fs")),
        check_vma=False,
    )
```
